256 devices in a mesh: grp: 4 (over y, x), ep: 32 (over z), tp: 2 (over core).
Axes of the slice: x: 2, y: 2, z: 32, core: 2. Of those that a mesh axis runs over, the one named last changes fastest.
The devices are a block of a 4x8x32 slice.
Arguments:
- tokens: bfloat16 [16384, 4096], P(('grp', 'ep')), parts along dimension 0, may hold values from -16 to 16, as said below
- norm_gain: float32 [4096], replicated, may hold values from 0.1 to 1.9
- gate_weight: bfloat16 [32, 4096, 768], P('ep', None, 'tp'), may hold values from -0.09375 to 0.09375
- up_weight: bfloat16 [32, 4096, 768], P('ep', None, 'tp'), may hold values from -0.09375 to 0.09375
- down_weight: bfloat16 [32, 768, 4096], P('ep', 'tp'), may hold values from -0.21875 to 0.21875
- chosen: int32 [128, 32, 20], P(('grp', 'ep')), parts along dimension 0, may hold values from 0 to 128, as said below
- affinity: float32 [128, 32, 20], P(('grp', 'ep')), parts along dimension 0, may hold values from 0.2 to 1
Outputs:
- mixed: bfloat16 [16384, 4096], P(('grp', 'ep'), 'tp'), parts along dimension 0
The draws below stay inside these ranges and needn't reach their ends.
There are 4 independent parts, one for each index of `grp`. The reference program is written for one: setup_inputs(seed, part) draws one part's arguments, and reference() takes and returns one part's arrays. A program takes and returns all parts, laid end to end along the dimension named above; an argument that names none is the same for every part. Nothing has to cross between parts.
Inputs may be any that keep to these rules, and one draw needn't show every extreme that they name: `tokens`: draws differ in their scale from row to row. `chosen`: in each (block, expert) row the live entries come first and are distinct; dead entries equal 128. Every expert has exactly 512 live slots in all and at least one live slot in every block; some block gives some expert exactly 20 live slots.
All inputs are finite; a program needn't handle non-finite values.
Results may differ from the reference program's by a relative error of at most 0.0095.
Values may be sent and summed in bfloat16 or wider, within the bound.
A program may use at most 64 MiB of HBM per device.

```python
import math
import jax
import jax.numpy as jnp
from jax import lax

D = 4096
FF = 768
TOK_DEV = 128
TOKENS = 4096
EXPERTS = 32
SLOT = 20
N_EP = 32
N_TP = 2


def draw_tokens(key, part):
    first_key, second_key = jax.random.split(key)
    base = jnp.clip(jax.random.normal(first_key, (TOKENS, D), jnp.float32), -4.0, 4.0)
    row_scale = jnp.exp(jax.random.uniform(second_key, (TOKENS, 1), jnp.float32, math.log(0.3), math.log(3.0)))
    return (base * row_scale).astype(jnp.bfloat16)


def draw_chosen(key, part):
    half_axis = N_EP // 2
    average = TOK_DEV // 8
    spread = SLOT - average
    keys = jax.random.split(key, 4)
    delta = jax.random.randint(keys[0], (EXPERTS, half_axis), 0, spread + 1)
    forced = jax.random.randint(keys[1], (EXPERTS, 1), 0, half_axis)
    delta = jnp.where(jnp.arange(half_axis)[None, :] == forced, spread, delta)
    signs = jax.random.randint(keys[2], (EXPERTS, half_axis), 0, 2) * 2 - 1
    counts = jnp.concatenate([average + signs * delta, average - signs * delta], axis=1)
    per_block = jnp.transpose(counts)
    scores = jax.random.randint(keys[3], (N_EP, EXPERTS, TOK_DEV), 0, 1 << 20) * TOK_DEV + jnp.arange(TOK_DEV)[None, None, :]
    order = jnp.argsort(scores, axis=-1, stable=True)[:, :, :SLOT]
    picks = jnp.where(jnp.arange(SLOT)[None, None, :] < per_block[:, :, None], order, TOK_DEV)
    return picks.astype(jnp.int32)


def steps_of(own_key, extent, pieces, smallest, high):
    factor_of = 1.0
    for position, blocks in pieces:
        heights = jax.random.uniform(jax.random.fold_in(jax.random.fold_in(own_key, 6), position), (blocks,), jnp.float32, smallest / len(pieces), high / len(pieces))
        factor_of = factor_of * jnp.repeat(jnp.exp(heights), extent[position] // blocks).reshape((-1,) + (1,) * (len(extent) - 1 - position))
    return factor_of


def normal_values(key, shape, scale, reach, pieces=(), kind=jnp.bfloat16):
    values = scale * jax.random.normal(key, shape, jnp.float32)
    if pieces:
        values = values * steps_of(key, shape, pieces, -0.22, 0.18)
    return jnp.clip(values, -reach, reach).astype(kind)


def setup_inputs(seed: int = 0, part: int = 0) -> dict:
    seeds = jax.random.split(jax.random.key(seed), 8)
    part_splits = jax.random.split(jax.random.fold_in(seeds[7], part), 8)
    return {
        "tokens": draw_tokens(jax.random.fold_in(jax.random.fold_in(seeds[7], part), 71), part),
        "norm_gain": jnp.clip(1.0 + 0.18 * jax.random.normal(seeds[1], (D,), jnp.float32), 0.1, 1.9),
        "gate_weight": normal_values(seeds[2], (EXPERTS, D, FF), D ** -0.5, 0.09375, ((0, 32), (2, 2))),
        "up_weight": normal_values(seeds[3], (EXPERTS, D, FF), D ** -0.5, 0.09375, ((0, 32), (2, 2))),
        "down_weight": normal_values(seeds[4], (EXPERTS, FF, D), FF ** -0.5, 0.21875, ((0, 32), (1, 2))),
        "chosen": draw_chosen(jax.random.fold_in(jax.random.fold_in(seeds[7], part), 71), part),
        "affinity": jnp.clip(0.2 + 0.8 * jax.random.uniform(part_splits[6], (N_EP, EXPERTS, SLOT), jnp.float32) ** steps_of(part_splits[6], (N_EP, EXPERTS, SLOT), ((0, 32),), -0.2, 0.2), 0.2, 1.0),
    }


norm_eps = 1e-06

def normalize(block, norm_gain):
    values = block.astype(jnp.float32)
    scaled = values * lax.rsqrt(lax.optimization_barrier(jnp.mean(values * values, axis=-1, keepdims=True)) + norm_eps)
    return (scaled * norm_gain.astype(jnp.float32)).astype(jnp.bfloat16)

def reference(tokens, norm_gain, gate_weight, up_weight, down_weight, chosen, affinity):
    total_rows = tokens.shape[0]
    model_width = tokens.shape[1]
    normed = normalize(tokens, norm_gain)
    ff_block = FF // N_TP
    block_base = jnp.arange(N_EP, dtype=jnp.int32)[:, None] * TOK_DEV

    def expert_step(carry, index):
        picks = chosen[:, index, :]
        live = picks < TOK_DEV
        global_rows = (block_base + jnp.minimum(picks, TOK_DEV - 1)).reshape(-1).astype(jnp.int32)
        picked = normed[global_rows]
        gate_proj = jnp.dot(picked, gate_weight[index], preferred_element_type=jnp.float32)
        up_value = jnp.dot(picked, up_weight[index], preferred_element_type=jnp.float32)
        hidden = (jax.nn.silu(gate_proj) * up_value).astype(jnp.bfloat16)
        partial_sum = jnp.zeros((picked.shape[0], model_width), jnp.float32)
        for piece_index in range(N_TP):
            lower = piece_index * ff_block
            piece = jnp.dot(hidden[:, lower:lower + ff_block], down_weight[index, lower:lower + ff_block], preferred_element_type=jnp.float32)
            partial_sum = partial_sum + piece.astype(jnp.bfloat16).astype(jnp.float32)
        expert_out = partial_sum.astype(jnp.bfloat16)
        weight = jnp.where(live, affinity[:, index, :], 0.0).astype(jnp.bfloat16).reshape(-1)
        contrib = weight.astype(jnp.float32)[:, None] * expert_out.astype(jnp.float32)
        target = jnp.where(live.reshape(-1), global_rows, total_rows).astype(jnp.int32)
        return (carry.at[target].add(contrib, mode='drop'), None)
    start_sum = jnp.zeros((total_rows, model_width), jnp.float32)
    result, unused = lax.scan(expert_step, start_sum, jnp.arange(chosen.shape[1], dtype=jnp.int32))
    return result.astype(jnp.bfloat16)
```

```python
import functools

import jax
import jax.numpy as jnp
from jax import lax
from jax.experimental import pallas as pl
from jax.experimental.pallas import tpu as pltpu
from jax.sharding import PartitionSpec as P

norm_eps = 1e-06
UNIT = 32
REACH = 11
CHUNKS = 4
f32, bf16 = jnp.float32, jnp.bfloat16


def up8(rows):
    return -(-rows // 8) * 8


def dot(a, b):
    return jnp.dot(a, b, preferred_element_type=f32)


def dot_rows(a, b):
    return lax.dot_general(a, b, (((0,), (0,)), ((), ())), preferred_element_type=f32)


def kernel(
    n, reach, slots, tokens, gain, meta, gate_hbm, up_hbm, down_hbm, out,
    own, ring, mring, w_own, w_oth, d_own, d_oth, pk_own, pk_oth, eo, ps, po, psf, pof,
    far_out, far_in, red, top,
    wsem, dsend, drecv, msend, mrecv, pxs, pxr, pas, par, fs, fr, gs, gr, rs, rr,
):
    me, core = lax.axis_index("ep"), lax.axis_index("tp")
    far = n // 2 - reach
    chunks, trows, width = own.shape
    half = chunks * width
    hid = w_own.shape[1] // 2
    full_rows = up8(slots)
    base = slots // 2 // 8 * 8
    end_rows = up8(max(slots // 2, slots - base))
    partner = {"tp": 1 - core}
    sign = (1, -1)

    def at(offset):
        return {"ep": lax.rem(me + offset + n, n)}

    def rcopy(src, dst, s, r, dev):
        return pltpu.make_async_remote_copy(
            src_ref=src, dst_ref=dst, send_sem=s, recv_sem=r, device_id=dev,
            device_id_type=pl.DeviceIdType.MESH,
        )

    def far_rows(j):
        return full_rows if j < far else end_rows

    def hop(d, g, ch):
        src = own.at[ch] if d is None else ring.at[g, d, ch]
        nxt = 0 if d is None else d + 1
        return rcopy(src, ring.at[g, nxt, ch], dsend.at[g, nxt, ch], drecv.at[g, nxt, ch], at(sign[g]))

    def landed(d, g, ch):
        return rcopy(own.at[ch], ring.at[g, d, ch], dsend.at[g, d, ch], drecv.at[g, d, ch], at(sign[g]))

    def mhop(d, g):
        src = meta if d is None else mring.at[g, d]
        nxt = 0 if d is None else d + 1
        return rcopy(src, mring.at[g, nxt], msend.at[g, nxt], mrecv.at[g, nxt], at(sign[g]))

    def mlanded(d, g):
        return rcopy(meta, mring.at[g, d], msend.at[g, d], mrecv.at[g, d], at(sign[g]))

    def share(d):
        return rcopy(pk_own.at[d], pk_oth.at[d], pxs.at[d], pxr.at[d], partner)

    def give(src, d):
        return rcopy(src, eo.at[d], pas.at[d], par.at[d], partner)

    def far_send(g, j):
        rows = far_rows(j)
        return rcopy(
            far_out.at[g, j - 1, pl.ds(0, rows)], pk_own.at[reach + j, pl.ds(g * UNIT, rows)],
            fs.at[g, j - 1], fr.at[g, j - 1], at(sign[g] * j),
        )

    def far_back(g, j):
        rows = far_rows(j)
        return rcopy(
            eo.at[reach + j, pl.ds(g * UNIT, rows)], far_in.at[g, j - 1, pl.ds(0, rows)],
            gs.at[g, j - 1], gr.at[g, j - 1], at(-sign[g] * j),
        )

    def back(src, d, g, ch):
        return rcopy(src, red.at[g, d, ch], rs.at[g, d, ch], rr.at[g, d, ch], at(-sign[g]))

    lane = lax.broadcasted_iota(jnp.int32, (UNIT, meta.shape[1]), 1)
    tok = lax.broadcasted_iota(jnp.int32, (UNIT, trows), 1).astype(f32)
    slot = lax.broadcasted_iota(jnp.int32, (UNIT, 1), 0)

    def column(m, index):
        return jnp.sum(jnp.where(lane == index, m, 0.0), axis=1, keepdims=True)

    def hot(m, e, weighted, end=None):
        rows = column(m, e)
        value = column(m, n + e) if weighted else jnp.ones((UNIT, 1), f32)
        if end is not None:
            keep = (slot < slots // 2) if end == 0 else (slot >= slots // 2)
            rows = jnp.where(keep, rows, float(trows))
            if end == 1 and base:
                fill = jnp.full((base, 1), float(trows), f32)
                rows = jnp.concatenate([rows[base:], fill], axis=0)
                value = jnp.concatenate([value[base:], fill], axis=0)
        return jnp.where(rows == tok, value, 0.0)

    def far_hot(m, g, weighted):
        parts = []
        for j in range(1, far + 1):
            e = lax.rem(me + sign[g] * j + n, n)
            parts.append(hot(m, e, weighted, g if j == far else None))
        return jnp.concatenate(parts, axis=0).astype(bf16)

    loads = []
    for i, (src, dst) in enumerate((
        (gate_hbm.at[0, pl.ds(core * half, half)], w_own.at[:, pl.ds(0, hid)]),
        (up_hbm.at[0, pl.ds(core * half, half)], w_own.at[:, pl.ds(hid, hid)]),
        (gate_hbm.at[0, pl.ds((1 - core) * half, half)], w_oth.at[:, pl.ds(0, hid)]),
        (up_hbm.at[0, pl.ds((1 - core) * half, half)], w_oth.at[:, pl.ds(hid, hid)]),
        (down_hbm.at[0, :, pl.ds(pl.multiple_of(core * half, 128), half)], d_own),
        (down_hbm.at[0, :, pl.ds(pl.multiple_of((1 - core) * half, 128), half)], d_oth),
    )):
        loads.append(pltpu.make_async_copy(src, dst, wsem.at[i]))
        loads[-1].start()

    pk_own[0] = jnp.zeros_like(pk_own[0])
    for j in range(1, far + 1):
        pk_own[reach + j] = jnp.zeros_like(pk_own[reach + j])
        for g in range(2):
            far_in[g, j - 1] = jnp.zeros_like(far_in[g, j - 1])

    barrier = pltpu.get_barrier_semaphore()
    peers = [at(s * j) for j in range(1, far + 1) for s in sign] + [partner]
    for peer in peers:
        pl.semaphore_signal(barrier, inc=1, device_id=peer, device_id_type=pl.DeviceIdType.MESH)
    squares = jnp.zeros((trows, 1), f32)
    for i in range(2 * chunks):
        v = tokens[:, pl.ds(i * width, width)].astype(f32)
        squares += jnp.sum(v * v, axis=1, keepdims=True)
    scale = lax.rsqrt(squares / tokens.shape[1] + norm_eps)
    pl.semaphore_wait(barrier, len(peers))

    for g in range(2):
        mhop(None, g).start()
    for ch in range(chunks):
        cols = pl.ds(pl.multiple_of(core * half + ch * width, 128), width)
        own[ch] = (tokens[:, cols].astype(f32) * scale * gain[:, cols]).astype(bf16)
        for g in range(2):
            hop(None, g, ch).start()

    own_hot = hot(meta[...].astype(f32), me, False).astype(bf16)
    for ch in range(chunks):
        pk_own[0, pl.ds(0, UNIT), pl.ds(ch * width, width)] = dot(own_hot, own[ch]).astype(bf16)
    share(0).start()
    for load in loads:
        load.wait()

    def hidden_of(a, b):
        acc = dot(a, w_own[...]) + dot(b, w_oth[...])
        gate, upper = acc[:, :hid], acc[:, hid:]
        return (gate * jax.nn.sigmoid(gate) * upper).astype(bf16)

    def pick(t):
        for g in range(2):
            h = hot(mring[g, t - 1].astype(f32), me, False).astype(bf16)
            for ch in range(chunks):
                pk_own[t, pl.ds(g * UNIT, UNIT), pl.ds(ch * width, width)] = dot(h, ring[g, t - 1, ch]).astype(bf16)
        share(t).start()

    def pick_far():
        for g in range(2):
            h = far_hot(mring[g, reach - 1].astype(f32), g, False)
            for ch in range(chunks):
                y = dot(h, ring[g, reach - 1, ch]).astype(bf16)
                far_out[g, :, :, pl.ds(ch * width, width)] = y.reshape(far, UNIT, width)
        for j in range(far, 0, -1):
            for g in range(2):
                far_send(g, j).start()

    def expert(b):
        share(b).wait_recv()
        h = hidden_of(pk_own[b], pk_oth[b])
        spot = lax.rem(b, 2)

        @pl.when(b >= 2)
        def _():
            give(ps.at[spot], b - 2).wait_send()

        ps[spot] = dot(h, d_oth[...]).astype(bf16)
        give(ps.at[spot], b).start()
        po[spot] = dot(h, d_own[...]).astype(bf16)

    def finish(b):
        give(ps.at[0], b).wait_recv()
        eo[b] = (po[lax.rem(b, 2)].astype(f32) + eo[b].astype(f32)).astype(bf16)

    def step(t, carry):
        @pl.when(t <= reach)
        def _():
            for g in range(2):
                mlanded(t - 1, g).wait_recv()

                @pl.when(t < reach)
                def _():
                    mhop(t - 1, g).start()

        for ch in range(chunks):
            @pl.when(t <= reach)
            def _():
                for g in range(2):
                    landed(t - 1, g, ch).wait_recv()

                    @pl.when(t < reach)
                    def _():
                        hop(t - 1, g, ch).start()

            if ch == 0:
                @pl.when(t <= reach + 1)
                def _():
                    expert(t - 1)

            if ch == chunks - 2:
                @pl.when(t >= 2)
                def _():
                    finish(t - 2)

        @pl.when(t == reach)
        def _():
            pick_far()

        @pl.when(t <= reach)
        def _():
            pick(t)

        return carry

    lax.fori_loop(1, reach + 3, step, 0)

    for j in range(1, far + 1):
        for g in range(2):
            far_send(g, j).wait_recv()
        share(reach + j).start()
    for j in range(1, far + 1):
        share(reach + j).wait_recv()
    group = pl.ds(reach + 1, far)
    h = hidden_of(
        pk_own[group].reshape(far * 2 * UNIT, half), pk_oth[group].reshape(far * 2 * UNIT, half)
    )
    psf[...] = dot(h, d_oth[...]).astype(bf16).reshape(psf.shape)
    for j in range(far, 0, -1):
        give(psf.at[j - 1], reach + j).start()
    pof[...] = dot(h, d_own[...]).astype(bf16).reshape(pof.shape)
    for j in range(far, 0, -1):
        give(psf.at[j - 1], reach + j).wait_recv()
        eo[reach + j] = (pof[j - 1].astype(f32) + eo[reach + j].astype(f32)).astype(bf16)
        for g in range(2):
            far_back(g, j).start()

    own_w = hot(meta[...].astype(f32), me, True).astype(bf16)
    near_w = [hot(mring[g, reach - 1].astype(f32), me, True).astype(bf16) for g in range(2)]
    for j in range(far, 0, -1):
        for g in range(2):
            far_back(g, j).wait_recv()
    for g in range(2):
        fw = far_hot(mring[g, reach - 1].astype(f32), g, True)
        for ch in range(chunks):
            cols = pl.ds(ch * width, width)
            total = dot_rows(fw, far_in[g, :, :, cols].reshape(far * UNIT, width))
            total += dot_rows(near_w[g], eo[reach, pl.ds(g * UNIT, UNIT), cols])
            top[g, ch] = total.astype(bf16)
            back(top.at[g, ch], reach - 1, g, ch).start()

    def fold(i, carry):
        d = reach - i
        hots = [hot(mring[g, d - 1].astype(f32), me, True).astype(bf16) for g in range(2)]
        for ch in range(chunks):
            cols = pl.ds(ch * width, width)
            for g in range(2):
                add = dot_rows(hots[g], eo[d, pl.ds(g * UNIT, UNIT), cols])
                back(top.at[g, ch], d, g, ch).wait_recv()
                red[g, d, ch] = (red[g, d, ch].astype(f32) + add).astype(bf16)
                back(red.at[g, d, ch], d - 1, g, ch).start()
        return carry

    lax.fori_loop(1, reach, fold, 0)

    for ch in range(chunks):
        cols = pl.ds(ch * width, width)
        add = dot_rows(own_w, eo[0, pl.ds(0, UNIT), cols])
        for g in range(2):
            back(top.at[g, ch], 0, g, ch).wait_recv()
            add += red[g, 0, ch].astype(f32)
        out[:, cols] = add.astype(bf16)

    def drain(d, carry):
        for g in range(2):
            mlanded(d, g).wait_send()
            for ch in range(chunks):
                landed(d, g, ch).wait_send()
                back(top.at[g, ch], d, g, ch).wait_send()
        return carry

    lax.fori_loop(0, reach, drain, 0)

    def drain_share(d, carry):
        share(d).wait_send()
        return carry

    lax.fori_loop(0, reach + far + 1, drain_share, 0)
    for b in range(reach - 1, reach + 1):
        give(ps.at[0], b).wait_send()
    for j in range(1, far + 1):
        give(psf.at[j - 1], reach + j).wait_send()
        for g in range(2):
            far_send(g, j).wait_send()
            far_back(g, j).wait_send()


def shards(n, reach, chunks, tokens, norm_gain, gate_weight, up_weight, down_weight, chosen, affinity):
    trows, model = tokens.shape
    half = model // 2
    width = half // chunks
    slots = chosen.shape[2]
    hid = gate_weight.shape[2]
    far = n // 2 - reach
    picked = chosen[0]
    weight = jnp.where(picked < trows, affinity[0], 0.0)
    table = jnp.concatenate([picked.astype(f32), weight], axis=0).T
    table = jnp.pad(table, ((0, 0), (0, max(128, 2 * n) - 2 * n)))
    meta = jnp.pad(table, ((0, UNIT - slots), (0, 0)), constant_values=float(trows)).astype(bf16)
    dma, batches = pltpu.SemaphoreType.DMA, reach + far + 1
    vmem = pl.BlockSpec(memory_space=pltpu.VMEM)
    anywhere = pl.BlockSpec(memory_space=pl.ANY)
    return pl.pallas_call(
        functools.partial(kernel, n, reach, slots),
        out_shape=jax.ShapeDtypeStruct((trows, half), bf16),
        in_specs=[vmem] * 3 + [anywhere] * 3,
        out_specs=vmem,
        scratch_shapes=[
            pltpu.VMEM((chunks, trows, width), bf16),
            pltpu.VMEM((2, reach, chunks, trows, width), bf16),
            pltpu.VMEM((2, reach, UNIT, meta.shape[1]), bf16),
            pltpu.VMEM((half, 2 * hid), bf16),
            pltpu.VMEM((half, 2 * hid), bf16),
            pltpu.VMEM((hid, half), bf16),
            pltpu.VMEM((hid, half), bf16),
            pltpu.VMEM((batches, 2 * UNIT, half), bf16),
            pltpu.VMEM((batches, 2 * UNIT, half), bf16),
            pltpu.VMEM((batches, 2 * UNIT, half), bf16),
            pltpu.VMEM((2, 2 * UNIT, half), bf16),
            pltpu.VMEM((2, 2 * UNIT, half), bf16),
            pltpu.VMEM((far, 2 * UNIT, half), bf16),
            pltpu.VMEM((far, 2 * UNIT, half), bf16),
            pltpu.VMEM((2, far, UNIT, half), bf16),
            pltpu.VMEM((2, far, UNIT, half), bf16),
            pltpu.VMEM((2, reach, chunks, trows, width), bf16),
            pltpu.VMEM((2, chunks, trows, width), bf16),
            dma((6,)),
            dma((2, reach, chunks)), dma((2, reach, chunks)),
            dma((2, reach)), dma((2, reach)),
            dma((batches,)), dma((batches,)), dma((batches,)), dma((batches,)),
            dma((2, far)), dma((2, far)), dma((2, far)), dma((2, far)),
            dma((2, reach, chunks)), dma((2, reach, chunks)),
        ],
        compiler_params=pltpu.CompilerParams(
            collective_id=0, has_side_effects=True, vmem_limit_bytes=67043328
        ),
    )(tokens, norm_gain[None, :], meta, gate_weight, up_weight, down_weight)


def solution(mesh):
    n = mesh.shape["ep"]
    in_specs = (
        P(("grp", "ep"), None),
        P(),
        P("ep", None, "tp"),
        P("ep", None, "tp"),
        P("ep", "tp", None),
        P(("grp", "ep"), None, None),
        P(("grp", "ep"), None, None),
    )
    body = functools.partial(shards, n, min(REACH, n // 2 - 1), CHUNKS)
    return jax.shard_map(body, mesh=mesh, in_specs=in_specs, out_specs=P(("grp", "ep"), "tp"), check_vma=False)
```

```python
import functools

import jax
import jax.numpy as jnp
from jax import lax
from jax.experimental import pallas as pl
from jax.experimental.pallas import tpu as pltpu
from jax.sharding import PartitionSpec as P

norm_eps = 1e-06
UNIT = 32
REACH = 11
CHUNKS = 4
f32, bf16 = jnp.float32, jnp.bfloat16


def up8(rows):
    return -(-rows // 8) * 8


def dot(a, b):
    return jnp.dot(a, b, preferred_element_type=f32)


def dot_rows(a, b):
    return lax.dot_general(a, b, (((0,), (0,)), ((), ())), preferred_element_type=f32)


def kernel(
    n, reach, slots, tokens_hbm, gain_hbm, chosen_hbm, affinity_hbm, gate_hbm, up_hbm, down_hbm, out,
    tokens, gain, chosen, affinity, meta, own, ring, mring, w_own, w_oth, d_own, d_oth,
    pk_own, pk_oth, eo, ps, po, far_out, far_got, far_ret, far_in, red, top,
    wsem, dsend, drecv, msend, mrecv, pxs, pxr, pas, par, fs, fr, gs, gr, rs, rr,
):
    me, core = lax.axis_index("ep"), lax.axis_index("tp")
    far = n // 2 - reach
    chunks, trows, width = own.shape
    half = chunks * width
    hid = w_own.shape[1] // 2
    pack_rows = far_out.shape[3]
    end_rows = up8(2 * (slots - slots // 2))
    batches = reach + far + 1
    partner = {"tp": 1 - core}
    sign = (1, -1)

    def at(offset):
        return {"ep": lax.rem(me + offset + n, n)}

    def rcopy(src, dst, s, r, dev):
        return pltpu.make_async_remote_copy(
            src_ref=src, dst_ref=dst, send_sem=s, recv_sem=r, device_id=dev,
            device_id_type=pl.DeviceIdType.MESH,
        )

    def hop(d, g, ch):
        src = own.at[ch] if d is None else ring.at[g, d, ch]
        nxt = 0 if d is None else d + 1
        return rcopy(src, ring.at[g, nxt, ch], dsend.at[g, nxt, ch], drecv.at[g, nxt, ch], at(sign[g]))

    def landed(d, g, ch):
        return rcopy(own.at[ch], ring.at[g, d, ch], dsend.at[g, d, ch], drecv.at[g, d, ch], at(sign[g]))

    def mhop(d, g):
        src = meta if d is None else mring.at[g, d]
        nxt = 0 if d is None else d + 1
        return rcopy(src, mring.at[g, nxt], msend.at[g, nxt], mrecv.at[g, nxt], at(sign[g]))

    def mlanded(d, g):
        return rcopy(meta, mring.at[g, d], msend.at[g, d], mrecv.at[g, d], at(sign[g]))

    def share(d):
        return rcopy(pk_own.at[d], pk_oth.at[d], pxs.at[d], pxr.at[d], partner)

    def give(src, d):
        return rcopy(src, eo.at[d], pas.at[d], par.at[d], partner)

    def far_copy(src, dst, s, r, g, j, h, end, way):
        rows = pl.ds(0, end_rows if end else pack_rows)
        return rcopy(
            src.at[g, j - 1, h, rows], dst.at[g, j - 1, h, rows],
            s.at[g, j - 1, h], r.at[g, j - 1, h], at(way * sign[g] * j),
        )

    def far_send(g, j, h, end):
        return far_copy(far_out, far_got, fs, fr, g, j, h, end, 1)

    def far_back(g, j, h, end):
        return far_copy(far_ret, far_in, gs, gr, g, j, h, end, -1)

    def back(src, d, g, ch):
        return rcopy(src, red.at[g, d, ch], rs.at[g, d, ch], rr.at[g, d, ch], at(-sign[g]))

    lane = lax.broadcasted_iota(jnp.int32, (UNIT, meta.shape[1]), 1)
    tok = lax.broadcasted_iota(jnp.int32, (UNIT, trows), 1).astype(f32)
    slot = lax.broadcasted_iota(jnp.int32, (UNIT, 1), 0)

    def column(m, index):
        return jnp.sum(jnp.where(lane == index, m, 0.0), axis=1, keepdims=True)

    def hot(m, e, weighted):
        value = column(m, n + e) if weighted else 1.0
        return jnp.where(column(m, e) == tok, value, 0.0).astype(bf16)

    pack_r = lax.broadcasted_iota(jnp.int32, (pack_rows, UNIT), 0)
    pack_s = lax.broadcasted_iota(jnp.int32, (pack_rows, UNIT), 1)

    def packer(g, end):
        low = slots // 2
        count = jnp.where(end, low if g == 0 else slots - low, slots)
        first = jnp.where(end, 0 if g == 0 else low, 0)
        a = (pack_r < count) & (pack_s == pack_r + first)
        b = (pack_r >= count) & (pack_r < 2 * count) & (pack_s == pack_r - count + first)
        return [jnp.where(v, 1.0, 0.0).astype(bf16) for v in (a, b)]

    def far_hot(m, g, weighted):
        sides = [[], []]
        for j in range(1, far + 1):
            h = hot(m, lax.rem(me + sign[g] * j + n, n), weighted)
            for side, pk in zip(sides, packer(g, j == far)):
                side.append(dot(pk, h))
        return [jnp.concatenate(side, axis=0).astype(bf16) for side in sides]

    loads = []
    for i, (src, dst) in enumerate((
        (tokens_hbm, tokens),
        (gain_hbm, gain),
        (chosen_hbm.at[0], chosen),
        (affinity_hbm.at[0], affinity),
        (gate_hbm.at[0, pl.ds(core * half, half)], w_own.at[:, pl.ds(0, hid)]),
        (up_hbm.at[0, pl.ds(core * half, half)], w_own.at[:, pl.ds(hid, hid)]),
        (gate_hbm.at[0, pl.ds((1 - core) * half, half)], w_oth.at[:, pl.ds(0, hid)]),
        (up_hbm.at[0, pl.ds((1 - core) * half, half)], w_oth.at[:, pl.ds(hid, hid)]),
        (down_hbm.at[0, :, pl.ds(pl.multiple_of(core * half, 128), half)], d_own),
        (down_hbm.at[0, :, pl.ds(pl.multiple_of((1 - core) * half, 128), half)], d_oth),
    )):
        loads.append(pltpu.make_async_copy(src, dst, wsem.at[i]))
        loads[-1].start()

    barrier = pltpu.get_barrier_semaphore()
    peers = [at(s * j) for j in range(1, far + 1) for s in sign] + [partner]
    for peer in peers:
        pl.semaphore_signal(barrier, inc=1, device_id=peer, device_id_type=pl.DeviceIdType.MESH)

    for buf in (far_got, far_in):
        for g in range(2):
            for h in range(2):
                rest = pl.ds(end_rows, pack_rows - end_rows)
                buf[g, far - 1, h, rest] = jnp.zeros_like(buf[g, far - 1, h, rest])
    loads[0].wait()
    loads[1].wait()
    squares = jnp.zeros((trows, 1), f32)
    for i in range(2 * chunks):
        v = tokens[:, pl.ds(i * width, width)].astype(f32)
        squares += jnp.sum(v * v, axis=1, keepdims=True)
    scale = lax.rsqrt(squares / tokens.shape[1] + norm_eps)
    for ch in range(chunks):
        cols = pl.ds(pl.multiple_of(core * half + ch * width, 128), width)
        own[ch] = (tokens[:, cols].astype(f32) * scale * gain[:, cols]).astype(bf16)
    loads[2].wait()
    loads[3].wait()
    experts = chosen.shape[0]
    spread = lax.broadcasted_iota(jnp.int32, (UNIT, slots), 0) == lax.broadcasted_iota(jnp.int32, (UNIT, slots), 1)
    spread = jnp.where(spread, 1.0, 0.0).astype(bf16)
    e_row = lax.broadcasted_iota(jnp.int32, (experts, meta.shape[1]), 0)
    e_lane = lax.broadcasted_iota(jnp.int32, (experts, meta.shape[1]), 1)
    table = jnp.zeros(meta.shape, f32)
    for ref, shift in ((chosen, 0), (affinity, n)):
        turned = lax.dot_general(
            spread, ref[...].astype(f32).astype(bf16), (((1,), (1,)), ((), ())), preferred_element_type=f32
        )
        place = jnp.where(e_lane == e_row + shift, 1.0, 0.0).astype(bf16)
        table += dot(turned.astype(bf16), place)
    meta[...] = jnp.where(slot < slots, table, float(trows)).astype(bf16)
    pl.semaphore_wait(barrier, len(peers))

    for ch in range(chunks):
        for g in range(2):
            hop(None, g, ch).start()
            if ch == 0:
                mhop(None, g).start()
    pk_own[0, pl.ds(UNIT, UNIT)] = jnp.zeros_like(pk_own[0, pl.ds(UNIT, UNIT)])
    own_hot = hot(meta[...].astype(f32), me, False)
    for ch in range(chunks):
        pk_own[0, pl.ds(0, UNIT), pl.ds(ch * width, width)] = dot(own_hot, own[ch]).astype(bf16)
    share(0).start()
    for load in loads[4:]:
        load.wait()

    def hidden_of(a, b):
        acc = dot(a, w_own[...]) + dot(b, w_oth[...])
        gate, upper = acc[:, :hid], acc[:, hid:]
        return (gate * jax.nn.sigmoid(gate) * upper).astype(bf16)

    def pick(t):
        for g in range(2):
            h = hot(mring[g, t - 1].astype(f32), me, False)
            for ch in range(chunks):
                pk_own[t, pl.ds(g * UNIT, UNIT), pl.ds(ch * width, width)] = dot(h, ring[g, t - 1, ch]).astype(bf16)
        share(t).start()

    def pick_far(h):
        for g in range(2):
            pa, pb = far_hot(mring[g, reach - 1].astype(f32), g, False)
            left = dot(pa, ring[g, reach - 1, 2 * h]) + dot(pb, ring[g, reach - 1, 2 * h + 1])
            for j in range(1, far + 1):
                far_out[g, j - 1, h] = left[(j - 1) * pack_rows : j * pack_rows].astype(bf16)
        for j in range(far, 0, -1):
            for g in range(2):
                far_send(g, j, h, j == far).start()

    def turn(b):
        return jnp.where(b <= reach, b, 2 * reach + far + 1 - b)

    unturn = turn

    def expert(b):
        share(b).wait_recv()
        h = hidden_of(pk_own[b], pk_oth[b])
        spot = lax.rem(turn(b), 2)

        @pl.when(turn(b) >= 2)
        def _():
            give(ps.at[spot], unturn(turn(b) - 2)).wait_send()

        ps[spot] = dot(h, d_oth[...]).astype(bf16)
        give(ps.at[spot], b).start()
        po[spot] = dot(h, d_own[...]).astype(bf16)

    def finish(b):
        give(ps.at[0], b).wait_recv()
        eo[b] = (po[lax.rem(turn(b), 2)].astype(f32) + eo[b].astype(f32)).astype(bf16)

    def step(t, carry):
        @pl.when(t <= reach)
        def _():
            for g in range(2):
                mlanded(t - 1, g).wait_recv()

                @pl.when(t < reach)
                def _():
                    mhop(t - 1, g).start()

        for ch in range(chunks):
            @pl.when(t <= reach)
            def _():
                for g in range(2):
                    landed(t - 1, g, ch).wait_recv()

                    @pl.when(t < reach)
                    def _():
                        hop(t - 1, g, ch).start()

            if ch % 2:
                @pl.when(t == reach)
                def _():
                    pick_far(ch // 2)

            if ch == 0:
                @pl.when(t <= reach + 1)
                def _():
                    expert(t - 1)

            if ch == chunks - 2:
                @pl.when(t >= 2)
                def _():
                    finish(t - 2)

        @pl.when(t <= reach)
        def _():
            pick(t)

        return carry

    lax.fori_loop(1, reach + 3, step, 0)

    def far_step(i, carry):
        j = far - i

        @pl.when(i == 0)
        def _():
            for g in range(2):
                for h in range(2):
                    far_send(g, far, h, True).wait_recv()

        @pl.when((i > 0) & (i < far))
        def _():
            for g in range(2):
                for h in range(2):
                    far_send(g, j, h, False).wait_recv()

        @pl.when(i < far)
        def _():
            for g in range(2):
                pks = packer(g, i == 0)
                for ch in range(chunks):
                    rows = dot_rows(pks[ch % 2], far_got[g, j - 1, ch // 2])
                    pk_own[reach + j, pl.ds(g * UNIT, UNIT), pl.ds(ch * width, width)] = rows.astype(bf16)
            share(reach + j).start()

        @pl.when((i > 0) & (i <= far))
        def _():
            expert(reach + j + 1)

        @pl.when(i > 1)
        def _():
            finish(reach + j + 2)
            for g in range(2):
                pks = packer(g, i == 2)
                for h in range(2):
                    y = dot(pks[0], eo[reach + j + 2, pl.ds(g * UNIT, UNIT), pl.ds(2 * h * width, width)])
                    y += dot(pks[1], eo[reach + j + 2, pl.ds(g * UNIT, UNIT), pl.ds((2 * h + 1) * width, width)])
                    far_ret[g, j + 1, h] = y.astype(bf16)

        @pl.when(i == 2)
        def _():
            for h in range(2):
                for g in range(2):
                    far_back(g, far, h, True).start()

        @pl.when(i > 2)
        def _():
            for g in range(2):
                far_back(g, j + 2, 0, False).start()

        return carry

    lax.fori_loop(0, far + 2, far_step, 0)
    for j in range(far - 1, 0, -1):
        for g in range(2):
            far_back(g, j, 1, False).start()

    own_w = hot(meta[...].astype(f32), me, True)
    near_w = [hot(mring[g, reach - 1].astype(f32), me, True) for g in range(2)]
    far_w = [far_hot(mring[g, reach - 1].astype(f32), g, True) for g in range(2)]
    for h in range(2):
        for j in range(far, 0, -1):
            for g in range(2):
                far_back(g, j, h, j == far).wait_recv()
        for ch in (2 * h, 2 * h + 1):
            cols = pl.ds(ch * width, width)
            for g in range(2):
                total = dot_rows(near_w[g], eo[reach, pl.ds(g * UNIT, UNIT), cols])
                for j in range(1, far + 1):
                    rows = far_w[g][ch % 2][(j - 1) * pack_rows : j * pack_rows]
                    total += dot_rows(rows, far_in[g, j - 1, h])
                top[g, ch] = total.astype(bf16)
                back(top.at[g, ch], reach - 1, g, ch).start()

    def fold(i, carry):
        d = reach - i
        hots = [hot(mring[g, d - 1].astype(f32), me, True) for g in range(2)]
        for ch in range(chunks):
            cols = pl.ds(ch * width, width)
            for g in range(2):
                add = dot_rows(hots[g], eo[d, pl.ds(g * UNIT, UNIT), cols])
                back(top.at[g, ch], d, g, ch).wait_recv()
                red[g, d, ch] = (red[g, d, ch].astype(f32) + add).astype(bf16)
                back(red.at[g, d, ch], d - 1, g, ch).start()
        return carry

    lax.fori_loop(1, reach, fold, 0)

    for ch in range(chunks):
        cols = pl.ds(ch * width, width)
        add = dot_rows(own_w, eo[0, pl.ds(0, UNIT), cols])
        for g in range(2):
            back(top.at[g, ch], 0, g, ch).wait_recv()
            add += red[g, 0, ch].astype(f32)
        out[:, cols] = add.astype(bf16)

    def drain(d, carry):
        for g in range(2):
            mlanded(d, g).wait_send()
            for ch in range(chunks):
                landed(d, g, ch).wait_send()
                back(top.at[g, ch], d, g, ch).wait_send()
        return carry

    lax.fori_loop(0, reach, drain, 0)

    def drain_share(d, carry):
        share(d).wait_send()
        return carry

    lax.fori_loop(0, batches, drain_share, 0)
    for b in (reach + 1, reach + 2) if far > 1 else (reach, reach + 1):
        give(ps.at[0], b).wait_send()
    for j in range(1, far + 1):
        for g in range(2):
            for h in range(2):
                far_send(g, j, h, j == far).wait_send()
                far_back(g, j, h, j == far).wait_send()


def shards(n, reach, chunks, tokens, norm_gain, gate_weight, up_weight, down_weight, chosen, affinity):
    trows, model = tokens.shape
    half = model // 2
    width = half // chunks
    slots = chosen.shape[2]
    hid = gate_weight.shape[2]
    far = n // 2 - reach
    pack_rows = up8(2 * slots)
    lanes = max(128, 2 * n)
    dma, batches = pltpu.SemaphoreType.DMA, reach + far + 1
    vmem = pl.BlockSpec(memory_space=pltpu.VMEM)
    anywhere = pl.BlockSpec(memory_space=pl.ANY)
    return pl.pallas_call(
        functools.partial(kernel, n, reach, slots),
        out_shape=jax.ShapeDtypeStruct((trows, half), bf16),
        in_specs=[anywhere] * 7,
        out_specs=vmem,
        scratch_shapes=[
            pltpu.VMEM((trows, model), bf16),
            pltpu.VMEM((1, model), f32),
            pltpu.VMEM(chosen.shape[1:], jnp.int32),
            pltpu.VMEM(chosen.shape[1:], f32),
            pltpu.VMEM((UNIT, lanes), bf16),
            pltpu.VMEM((chunks, trows, width), bf16),
            pltpu.VMEM((2, reach, chunks, trows, width), bf16),
            pltpu.VMEM((2, reach, UNIT, lanes), bf16),
            pltpu.VMEM((half, 2 * hid), bf16),
            pltpu.VMEM((half, 2 * hid), bf16),
            pltpu.VMEM((hid, half), bf16),
            pltpu.VMEM((hid, half), bf16),
            pltpu.VMEM((batches, 2 * UNIT, half), bf16),
            pltpu.VMEM((batches, 2 * UNIT, half), bf16),
            pltpu.VMEM((batches, 2 * UNIT, half), bf16),
            pltpu.VMEM((2, 2 * UNIT, half), bf16),
            pltpu.VMEM((2, 2 * UNIT, half), bf16),
            pltpu.VMEM((2, far, 2, pack_rows, width), bf16),
            pltpu.VMEM((2, far, 2, pack_rows, width), bf16),
            pltpu.VMEM((2, far, 2, pack_rows, width), bf16),
            pltpu.VMEM((2, far, 2, pack_rows, width), bf16),
            pltpu.VMEM((2, reach, chunks, trows, width), bf16),
            pltpu.VMEM((2, chunks, trows, width), bf16),
            dma((10,)),
            dma((2, reach, chunks)), dma((2, reach, chunks)),
            dma((2, reach)), dma((2, reach)),
            dma((batches,)), dma((batches,)), dma((batches,)), dma((batches,)),
            dma((2, far, 2)), dma((2, far, 2)), dma((2, far, 2)), dma((2, far, 2)),
            dma((2, reach, chunks)), dma((2, reach, chunks)),
        ],
        compiler_params=pltpu.CompilerParams(
            collective_id=0, has_side_effects=True, vmem_limit_bytes=67043328
        ),
    )(tokens, norm_gain[None, :], chosen, affinity, gate_weight, up_weight, down_weight)


def solution(mesh):
    n = mesh.shape["ep"]
    in_specs = (
        P(("grp", "ep"), None),
        P(),
        P("ep", None, "tp"),
        P("ep", None, "tp"),
        P("ep", "tp", None),
        P(("grp", "ep"), None, None),
        P(("grp", "ep"), None, None),
    )
    body = functools.partial(shards, n, min(REACH, n // 2 - 1), CHUNKS)
    return jax.shard_map(body, mesh=mesh, in_specs=in_specs, out_specs=P(("grp", "ep"), "tp"), check_vma=False)
```

```python
import functools

import jax
import jax.numpy as jnp
from jax import lax
from jax.experimental import pallas as pl
from jax.experimental.pallas import tpu as pltpu
from jax.sharding import PartitionSpec as P

norm_eps = 1e-06
UNIT = 32
REACH = 11
CHUNKS = 4
f32, bf16 = jnp.float32, jnp.bfloat16


def up8(rows):
    return -(-rows // 8) * 8


def dot(a, b):
    return jnp.dot(a, b, preferred_element_type=f32)


def dot_rows(a, b):
    return lax.dot_general(a, b, (((0,), (0,)), ((), ())), preferred_element_type=f32)


def kernel(
    n, reach, slots, tokens_hbm, gain_hbm, chosen_hbm, affinity_hbm, gate_hbm, up_hbm, down_hbm, out,
    tokens, gain, chosen, affinity, meta, own, ring, mring, w_own, w_oth, d_own, d_oth,
    pk_own, pk_oth, eo, ps, po, psf, pof, far_out, far_got, far_ret, far_in, red, top,
    wsem, dsend, drecv, msend, mrecv, pxs, pxr, pas, par, fs, fr, gs, gr, rs, rr,
):
    me, core = lax.axis_index("ep"), lax.axis_index("tp")
    far = n // 2 - reach
    chunks, trows, width = own.shape
    half = chunks * width
    hid = w_own.shape[1] // 2
    pack_rows = far_out.shape[3]
    batches = reach + far + 1
    partner = {"tp": 1 - core}
    sign = (1, -1)

    def at(offset):
        return {"ep": lax.rem(me + offset + n, n)}

    def rcopy(src, dst, s, r, dev):
        return pltpu.make_async_remote_copy(
            src_ref=src, dst_ref=dst, send_sem=s, recv_sem=r, device_id=dev,
            device_id_type=pl.DeviceIdType.MESH,
        )

    def hop(d, g, ch):
        src = own.at[ch] if d is None else ring.at[g, d, ch]
        nxt = 0 if d is None else d + 1
        return rcopy(src, ring.at[g, nxt, ch], dsend.at[g, nxt, ch], drecv.at[g, nxt, ch], at(sign[g]))

    def landed(d, g, ch):
        return rcopy(own.at[ch], ring.at[g, d, ch], dsend.at[g, d, ch], drecv.at[g, d, ch], at(sign[g]))

    def mhop(d, g):
        src = meta if d is None else mring.at[g, d]
        nxt = 0 if d is None else d + 1
        return rcopy(src, mring.at[g, nxt], msend.at[g, nxt], mrecv.at[g, nxt], at(sign[g]))

    def mlanded(d, g):
        return rcopy(meta, mring.at[g, d], msend.at[g, d], mrecv.at[g, d], at(sign[g]))

    def share(d):
        return rcopy(pk_own.at[d], pk_oth.at[d], pxs.at[d], pxr.at[d], partner)

    def give(src, d):
        return rcopy(src, eo.at[d], pas.at[d], par.at[d], partner)

    def far_copy(src, dst, s, r, g, j, h, way):
        return rcopy(
            src.at[g, h, j - 1], dst.at[g, h, j - 1], s.at[g, h, j - 1], r.at[g, h, j - 1], at(way * sign[g] * j)
        )

    def far_send(g, j, h):
        return far_copy(far_out, far_got, fs, fr, g, j, h, 1)

    def far_back(g, j, h):
        return far_copy(far_ret, far_in, gs, gr, g, j, h, -1)

    def parts_of(j):
        return (0,) if j == far else (0, 1)

    def back(src, d, g, ch):
        return rcopy(src, red.at[g, d, ch], rs.at[g, d, ch], rr.at[g, d, ch], at(-sign[g]))

    lane = lax.broadcasted_iota(jnp.int32, (UNIT, meta.shape[1]), 1)
    tok = lax.broadcasted_iota(jnp.int32, (UNIT, trows), 1).astype(f32)
    slot = lax.broadcasted_iota(jnp.int32, (UNIT, 1), 0)

    def column(m, index):
        return jnp.sum(jnp.where(lane == index, m, 0.0), axis=1, keepdims=True)

    def hot(m, e, weighted):
        value = column(m, n + e) if weighted else 1.0
        return jnp.where(column(m, e) == tok, value, 0.0).astype(bf16)

    pack_r = lax.broadcasted_iota(jnp.int32, (pack_rows, UNIT), 0)
    pack_s = lax.broadcasted_iota(jnp.int32, (pack_rows, UNIT), 1)

    def packer(g, end, ch):
        low = slots // 2
        count, first, place = slots, 0, ch % 2
        if end:
            count, first, place = (low, 0, ch) if g == 0 else (slots - low, low, ch)
        local = pack_r - place * count
        keep = (local >= 0) & (local < count) & (pack_s == local + first)
        return jnp.where(keep, 1.0, 0.0).astype(bf16)

    def part(j, ch):
        return 0 if j == far else ch // 2

    def far_hot(m, g, weighted):
        hots = [hot(m, lax.rem(me + sign[g] * j + n, n), weighted) for j in range(1, far + 1)]
        sides = []
        for ch in range(2 if far > 1 else 0):
            pk = packer(g, False, ch)
            sides.append(jnp.concatenate([dot(pk, h) for h in hots[:-1]], axis=0).astype(bf16))
        ends = [dot(packer(g, True, ch), hots[-1]).astype(bf16) for ch in range(chunks)]
        return sides, ends

    loads = []
    for i, (src, dst) in enumerate((
        (tokens_hbm, tokens),
        (gain_hbm, gain),
        (chosen_hbm, chosen),
        (affinity_hbm, affinity),
        (gate_hbm.at[0, pl.ds(core * half, half)], w_own.at[:, pl.ds(0, hid)]),
        (up_hbm.at[0, pl.ds(core * half, half)], w_own.at[:, pl.ds(hid, hid)]),
        (gate_hbm.at[0, pl.ds((1 - core) * half, half)], w_oth.at[:, pl.ds(0, hid)]),
        (up_hbm.at[0, pl.ds((1 - core) * half, half)], w_oth.at[:, pl.ds(hid, hid)]),
        (down_hbm.at[0, :, pl.ds(pl.multiple_of(core * half, 128), half)], d_own),
        (down_hbm.at[0, :, pl.ds(pl.multiple_of((1 - core) * half, 128), half)], d_oth),
    )):
        loads.append(pltpu.make_async_copy(src, dst, wsem.at[i]))
        loads[-1].start()

    barrier = pltpu.get_barrier_semaphore()
    peers = [at(1), at(-1), partner]
    for peer in peers:
        pl.semaphore_signal(barrier, inc=1, device_id=peer, device_id_type=pl.DeviceIdType.MESH)

    loads[0].wait()
    loads[1].wait()
    squares = jnp.zeros((trows, 1), f32)
    for i in range(2 * chunks):
        v = tokens[:, pl.ds(i * width, width)].astype(f32)
        squares += jnp.sum(v * v, axis=1, keepdims=True)
    scale = lax.rsqrt(squares / tokens.shape[1] + norm_eps)
    for ch in range(chunks):
        cols = pl.ds(pl.multiple_of(core * half + ch * width, 128), width)
        own[ch] = (tokens[:, cols].astype(f32) * scale * gain[:, cols]).astype(bf16)
    loads[2].wait()
    loads[3].wait()
    experts = chosen.shape[2]
    spread = lax.broadcasted_iota(jnp.int32, (UNIT, slots), 0) == lax.broadcasted_iota(jnp.int32, (UNIT, slots), 1)
    spread = jnp.where(spread, 1.0, 0.0).astype(bf16)
    e_row = lax.broadcasted_iota(jnp.int32, (experts, meta.shape[1]), 0)
    e_lane = lax.broadcasted_iota(jnp.int32, (experts, meta.shape[1]), 1)
    table = jnp.zeros((slots, meta.shape[1]), f32)
    for ref, shift in ((chosen, 0), (affinity, n)):
        place = jnp.where(e_lane == e_row + shift, 1.0, 0.0).astype(bf16)
        table += dot(ref[:, 0, :].astype(f32).astype(bf16), place)
    table = dot(spread, table.astype(bf16))
    meta[...] = jnp.where(slot < slots, table, float(trows)).astype(bf16)
    pl.semaphore_wait(barrier, len(peers))

    for ch in range(chunks):
        for g in range(2):
            hop(None, g, ch).start()
            if ch == 0:
                mhop(None, g).start()
    pk_own[0, pl.ds(UNIT, UNIT)] = jnp.zeros_like(pk_own[0, pl.ds(UNIT, UNIT)])
    own_hot = hot(meta[...].astype(f32), me, False)
    for ch in range(chunks):
        pk_own[0, pl.ds(0, UNIT), pl.ds(ch * width, width)] = dot(own_hot, own[ch]).astype(bf16)
    share(0).start()
    for load in loads[4:]:
        load.wait()

    def hidden_of(a, b):
        acc = dot(a, w_own[...]) + dot(b, w_oth[...])
        gate, upper = acc[:, :hid], acc[:, hid:]
        return (gate * jax.nn.sigmoid(gate) * upper).astype(bf16)

    def pick(t):
        for g in range(2):
            h = hot(mring[g, t - 1].astype(f32), me, False)
            for ch in range(chunks):
                pk_own[t, pl.ds(g * UNIT, UNIT), pl.ds(ch * width, width)] = dot(h, ring[g, t - 1, ch]).astype(bf16)
        share(t).start()

    def pick_far(h):
        for g in range(2):
            sides, ends = far_hot(mring[g, reach - 1].astype(f32), g, False)
            if far > 1:
                y = dot(sides[0], ring[g, reach - 1, 2 * h]) + dot(sides[1], ring[g, reach - 1, 2 * h + 1])
                far_out[g, h, pl.ds(0, far - 1)] = y.astype(bf16).reshape(far - 1, pack_rows, width)
            if h == 1:
                y = sum(dot(ends[ch], ring[g, reach - 1, ch]) for ch in range(chunks))
                far_out[g, 0, far - 1] = y.astype(bf16)
        first = [(far - 1, 0)] if far > 1 else []
        rest = [(far, 0)] + ([(far - 1, 1)] if far > 1 else [])
        rest += [(j, p) for j in range(far - 2, 0, -1) for p in (0, 1)]
        for j, p in rest if h else first:
            for g in range(2):
                far_send(g, j, p).start()

    def expert(b):
        share(b).wait_recv()
        h = hidden_of(pk_own[b], pk_oth[b])
        spot = lax.rem(b, 2)

        @pl.when(b >= 2)
        def _():
            give(ps.at[spot], b - 2).wait_send()

        ps[spot] = dot(h, d_oth[...]).astype(bf16)
        give(ps.at[spot], b).start()
        po[spot] = dot(h, d_own[...]).astype(bf16)

    def finish(b):
        give(ps.at[0], b).wait_recv()
        eo[b] = (po[lax.rem(b, 2)].astype(f32) + eo[b].astype(f32)).astype(bf16)

    def step(t, carry):
        @pl.when(t <= reach)
        def _():
            for g in range(2):
                mlanded(t - 1, g).wait_recv()

                @pl.when(t < reach)
                def _():
                    mhop(t - 1, g).start()

        for ch in range(chunks):
            @pl.when(t <= reach)
            def _():
                for g in range(2):
                    landed(t - 1, g, ch).wait_recv()

                    @pl.when(t < reach)
                    def _():
                        hop(t - 1, g, ch).start()

            if ch % 2:
                @pl.when(t == reach)
                def _():
                    pick_far(ch // 2)

            if ch == 0:
                @pl.when(t <= reach + 1)
                def _():
                    expert(t - 1)

            if ch == chunks - 2:
                @pl.when(t >= 2)
                def _():
                    finish(t - 2)

        @pl.when(t <= reach)
        def _():
            pick(t)

        return carry

    lax.fori_loop(1, reach + 3, step, 0)

    def far_group(js):
        for j in js:
            for g in range(2):
                for p in parts_of(j):
                    far_send(g, j, p).wait_recv()
            for g in range(2):
                for ch in range(chunks):
                    rows = dot_rows(packer(g, j == far, ch), far_got[g, part(j, ch), j - 1])
                    pk_own[reach + j, pl.ds(g * UNIT, UNIT), pl.ds(ch * width, width)] = rows.astype(bf16)
            share(reach + j).start()
        for j in js:
            share(reach + j).wait_recv()
        low, count = min(js), len(js)
        group, rows = pl.ds(reach + low, count), count * 2 * UNIT
        h = hidden_of(pk_own[group].reshape(rows, half), pk_oth[group].reshape(rows, half))
        spots = pl.ds(low - 1, count)
        psf[spots] = dot(h, d_oth[...]).astype(bf16).reshape(count, 2 * UNIT, half)
        for j in js:
            give(psf.at[j - 1], reach + j).start()
        pof[spots] = dot(h, d_own[...]).astype(bf16).reshape(count, 2 * UNIT, half)
        for j in js:
            b = reach + j
            give(psf.at[j - 1], b).wait_recv()
            eo[b] = (pof[j - 1].astype(f32) + eo[b].astype(f32)).astype(bf16)
            for g in range(2):
                for p in parts_of(j):
                    y = jnp.zeros((pack_rows, width), f32)
                    for ch in range(chunks):
                        if part(j, ch) == p:
                            y += dot(packer(g, j == far, ch), eo[b, pl.ds(g * UNIT, UNIT), pl.ds(ch * width, width)])
                    far_ret[g, p, j - 1] = y.astype(bf16)
                far_back(g, j, 0).start()
        for j in js:
            if j != far:
                for g in range(2):
                    far_back(g, j, 1).start()

    order = list(range(far, 0, -1))
    far_group(order[:2])
    if far > 2:
        far_group(order[2:])

    own_w = hot(meta[...].astype(f32), me, True)
    near_w = [hot(mring[g, reach - 1].astype(f32), me, True) for g in range(2)]
    far_w = [far_hot(mring[g, reach - 1].astype(f32), g, True) for g in range(2)]
    for h in range(2):
        for j in order:
            if h in parts_of(j):
                for g in range(2):
                    far_back(g, j, h).wait_recv()
        for ch in (2 * h, 2 * h + 1):
            cols = pl.ds(ch * width, width)
            for g in range(2):
                sides, ends = far_w[g]
                total = dot_rows(near_w[g], eo[reach, pl.ds(g * UNIT, UNIT), cols])
                total += dot_rows(ends[ch], far_in[g, 0, far - 1])
                if far > 1:
                    total += dot_rows(sides[ch % 2], far_in[g, h, pl.ds(0, far - 1)].reshape((far - 1) * pack_rows, width))
                top[g, ch] = total.astype(bf16)
                back(top.at[g, ch], reach - 1, g, ch).start()

    def fold(i, carry):
        d = reach - i
        hots = [hot(mring[g, d - 1].astype(f32), me, True) for g in range(2)]
        for ch in range(chunks):
            cols = pl.ds(ch * width, width)
            for g in range(2):
                add = dot_rows(hots[g], eo[d, pl.ds(g * UNIT, UNIT), cols])
                back(top.at[g, ch], d, g, ch).wait_recv()
                red[g, d, ch] = (red[g, d, ch].astype(f32) + add).astype(bf16)
                back(red.at[g, d, ch], d - 1, g, ch).start()
        return carry

    lax.fori_loop(1, reach, fold, 0)

    for ch in range(chunks):
        cols = pl.ds(ch * width, width)
        add = dot_rows(own_w, eo[0, pl.ds(0, UNIT), cols])
        for g in range(2):
            back(top.at[g, ch], 0, g, ch).wait_recv()
            add += red[g, 0, ch].astype(f32)
        out[:, cols] = add.astype(bf16)

    def drain(d, carry):
        for g in range(2):
            mlanded(d, g).wait_send()
            for ch in range(chunks):
                landed(d, g, ch).wait_send()
                back(top.at[g, ch], d, g, ch).wait_send()
        return carry

    lax.fori_loop(0, reach, drain, 0)

    def drain_share(d, carry):
        share(d).wait_send()
        return carry

    lax.fori_loop(0, batches, drain_share, 0)
    for b in (reach - 1, reach):
        give(ps.at[0], b).wait_send()
    for j in order:
        give(psf.at[j - 1], reach + j).wait_send()
        for g in range(2):
            for p in parts_of(j):
                far_send(g, j, p).wait_send()
                far_back(g, j, p).wait_send()


def shards(n, reach, chunks, tokens, norm_gain, gate_weight, up_weight, down_weight, chosen, affinity):
    trows, model = tokens.shape
    half = model // 2
    width = half // chunks
    slots = chosen.shape[2]
    hid = gate_weight.shape[2]
    far = n // 2 - reach
    pack_rows = up8(max(2 * slots, 4 * (slots - slots // 2)))
    chosen, affinity = [jnp.transpose(v, (2, 0, 1)) for v in (chosen, affinity)]
    lanes = max(128, 2 * n)
    dma, batches = pltpu.SemaphoreType.DMA, reach + far + 1
    vmem = pl.BlockSpec(memory_space=pltpu.VMEM)
    anywhere = pl.BlockSpec(memory_space=pl.ANY)
    return pl.pallas_call(
        functools.partial(kernel, n, reach, slots),
        out_shape=jax.ShapeDtypeStruct((trows, half), bf16),
        in_specs=[anywhere] * 7,
        out_specs=vmem,
        scratch_shapes=[
            pltpu.VMEM((trows, model), bf16),
            pltpu.VMEM((1, model), f32),
            pltpu.VMEM(chosen.shape, jnp.int32),
            pltpu.VMEM(chosen.shape, f32),
            pltpu.VMEM((UNIT, lanes), bf16),
            pltpu.VMEM((chunks, trows, width), bf16),
            pltpu.VMEM((2, reach, chunks, trows, width), bf16),
            pltpu.VMEM((2, reach, UNIT, lanes), bf16),
            pltpu.VMEM((half, 2 * hid), bf16),
            pltpu.VMEM((half, 2 * hid), bf16),
            pltpu.VMEM((hid, half), bf16),
            pltpu.VMEM((hid, half), bf16),
            pltpu.VMEM((batches, 2 * UNIT, half), bf16),
            pltpu.VMEM((batches, 2 * UNIT, half), bf16),
            pltpu.VMEM((batches, 2 * UNIT, half), bf16),
            pltpu.VMEM((2, 2 * UNIT, half), bf16),
            pltpu.VMEM((2, 2 * UNIT, half), bf16),
            pltpu.VMEM((far, 2 * UNIT, half), bf16),
            pltpu.VMEM((far, 2 * UNIT, half), bf16),
            pltpu.VMEM((2, 2, far, pack_rows, width), bf16),
            pltpu.VMEM((2, 2, far, pack_rows, width), bf16),
            pltpu.VMEM((2, 2, far, pack_rows, width), bf16),
            pltpu.VMEM((2, 2, far, pack_rows, width), bf16),
            pltpu.VMEM((2, reach, chunks, trows, width), bf16),
            pltpu.VMEM((2, chunks, trows, width), bf16),
            dma((10,)),
            dma((2, reach, chunks)), dma((2, reach, chunks)),
            dma((2, reach)), dma((2, reach)),
            dma((batches,)), dma((batches,)), dma((batches,)), dma((batches,)),
            dma((2, 2, far)), dma((2, 2, far)), dma((2, 2, far)), dma((2, 2, far)),
            dma((2, reach, chunks)), dma((2, reach, chunks)),
        ],
        compiler_params=pltpu.CompilerParams(
            collective_id=0, has_side_effects=True, vmem_limit_bytes=67043328
        ),
    )(tokens, norm_gain[None, :], chosen, affinity, gate_weight, up_weight, down_weight)


def solution(mesh):
    n = mesh.shape["ep"]
    in_specs = (
        P(("grp", "ep"), None),
        P(),
        P("ep", None, "tp"),
        P("ep", None, "tp"),
        P("ep", "tp", None),
        P(("grp", "ep"), None, None),
        P(("grp", "ep"), None, None),
    )
    body = functools.partial(shards, n, min(REACH, n // 2 - 1), CHUNKS)
    return jax.shard_map(body, mesh=mesh, in_specs=in_specs, out_specs=P(("grp", "ep"), "tp"), check_vma=False)
```

```python
import functools

import jax
import jax.numpy as jnp
from jax import lax
from jax.experimental import pallas as pl
from jax.experimental.pallas import tpu as pltpu
from jax.sharding import PartitionSpec as P

norm_eps = 1e-06
UNIT = 32
REACH = 10
CHUNKS = 4
f32, bf16 = jnp.float32, jnp.bfloat16


def up8(rows):
    return -(-rows // 8) * 8


def dot(a, b):
    return jnp.dot(a, b, preferred_element_type=f32)


def dot_rows(a, b):
    return lax.dot_general(a, b, (((0,), (0,)), ((), ())), preferred_element_type=f32)


def kernel(
    n, reach, slots, tokens_hbm, gain_hbm, chosen_hbm, affinity_hbm, gate_hbm, up_hbm, down_hbm, out,
    tokens, gain, chosen, affinity, meta, own, ring, mring, w_own, w_oth, d_own, d_oth,
    pk_own, pk_oth, eo, ps, po, psf, pof, far_out, far_got, far_ret, far_in, red, top,
    wsem, dsend, drecv, msend, mrecv, pxs, pxr, pas, par, fs, fr, gs, gr, rs, rr,
):
    me, core = lax.axis_index("ep"), lax.axis_index("tp")
    far = n // 2 - reach
    chunks, trows, width = own.shape
    half = chunks * width
    hid = w_own.shape[1] // 2
    pack_rows = far_out.shape[3]
    batches = reach + far + 1
    partner = {"tp": 1 - core}
    sign = (1, -1)

    def at(offset):
        return {"ep": lax.rem(me + offset + n, n)}

    def rcopy(src, dst, s, r, dev):
        return pltpu.make_async_remote_copy(
            src_ref=src, dst_ref=dst, send_sem=s, recv_sem=r, device_id=dev,
            device_id_type=pl.DeviceIdType.MESH,
        )

    def hop(d, g, ch):
        src = own.at[ch] if d is None else ring.at[g, d, ch]
        nxt = 0 if d is None else d + 1
        return rcopy(src, ring.at[g, nxt, ch], dsend.at[g, nxt, ch], drecv.at[g, nxt, ch], at(sign[g]))

    def landed(d, g, ch):
        return rcopy(own.at[ch], ring.at[g, d, ch], dsend.at[g, d, ch], drecv.at[g, d, ch], at(sign[g]))

    def mhop(d, g):
        src = meta if d is None else mring.at[g, d]
        nxt = 0 if d is None else d + 1
        return rcopy(src, mring.at[g, nxt], msend.at[g, nxt], mrecv.at[g, nxt], at(sign[g]))

    def mlanded(d, g):
        return rcopy(meta, mring.at[g, d], msend.at[g, d], mrecv.at[g, d], at(sign[g]))

    def share(d):
        return rcopy(pk_own.at[d], pk_oth.at[d], pxs.at[d], pxr.at[d], partner)

    def give(src, d):
        return rcopy(src, eo.at[d], pas.at[d], par.at[d], partner)

    def far_copy(src, dst, s, r, g, j, h, way):
        return rcopy(
            src.at[g, h, j - 1], dst.at[g, h, j - 1], s.at[g, h, j - 1], r.at[g, h, j - 1], at(way * sign[g] * j)
        )

    def far_send(g, j, h):
        return far_copy(far_out, far_got, fs, fr, g, j, h, 1)

    def far_back(g, j, h):
        return far_copy(far_ret, far_in, gs, gr, g, j, h, -1)

    def parts_of(j):
        return (0,) if j == far else (0, 1)

    def back(src, d, g, ch):
        return rcopy(src, red.at[g, d, ch], rs.at[g, d, ch], rr.at[g, d, ch], at(-sign[g]))

    low = slots // 2
    lane = lax.broadcasted_iota(jnp.int32, meta.shape, 1)
    tok = lax.broadcasted_iota(jnp.int32, (UNIT, trows), 1).astype(f32)

    def column(m, index):
        pair = [jnp.sum(jnp.where(lane == index + 2 * n * i, m, 0.0), axis=1, keepdims=True) for i in range(2)]
        return jnp.concatenate(pair, axis=0)

    def hot(m, e, weighted):
        value = column(m, n + e) if weighted else 1.0
        return jnp.where(column(m, e) == tok, value, 0.0).astype(bf16)

    pack_r = lax.broadcasted_iota(jnp.int32, (pack_rows, UNIT), 0)
    pack_s = lax.broadcasted_iota(jnp.int32, (pack_rows, UNIT), 1)

    def packer(g, end, ch):
        count, first, place = slots, 0, ch % 2
        if end:
            count, first, place = (low, 0, ch) if g == 0 else (slots - low, low, ch)
        local = pack_r - place * count
        wanted = local + first
        wanted = jnp.where(wanted < low, wanted, wanted - low + UNIT // 2)
        keep = (local >= 0) & (local < count) & (pack_s == wanted)
        return jnp.where(keep, 1.0, 0.0).astype(bf16)

    def part(j, ch):
        return 0 if j == far else ch // 2

    def far_hot(m, g, weighted):
        hots = [hot(m, lax.rem(me + sign[g] * j + n, n), weighted) for j in range(1, far + 1)]
        sides = []
        for ch in range(2 if far > 1 else 0):
            pk = packer(g, False, ch)
            sides.append(jnp.concatenate([dot(pk, h) for h in hots[:-1]], axis=0).astype(bf16))
        ends = [dot(packer(g, True, ch), hots[-1]).astype(bf16) for ch in range(chunks)]
        return sides, ends

    loads = []
    for i, (src, dst) in enumerate((
        (tokens_hbm, tokens),
        (gain_hbm, gain),
        (chosen_hbm, chosen),
        (affinity_hbm, affinity),
        (gate_hbm.at[0, pl.ds(core * half, half)], w_own.at[:, pl.ds(0, hid)]),
        (up_hbm.at[0, pl.ds(core * half, half)], w_own.at[:, pl.ds(hid, hid)]),
        (gate_hbm.at[0, pl.ds((1 - core) * half, half)], w_oth.at[:, pl.ds(0, hid)]),
        (up_hbm.at[0, pl.ds((1 - core) * half, half)], w_oth.at[:, pl.ds(hid, hid)]),
        (down_hbm.at[0, :, pl.ds(pl.multiple_of(core * half, 128), half)], d_own),
        (down_hbm.at[0, :, pl.ds(pl.multiple_of((1 - core) * half, 128), half)], d_oth),
    )):
        loads.append(pltpu.make_async_copy(src, dst, wsem.at[i]))
        loads[-1].start()

    barrier = pltpu.get_barrier_semaphore()
    peers = [at(1), at(-1), partner]
    for peer in peers:
        pl.semaphore_signal(barrier, inc=1, device_id=peer, device_id_type=pl.DeviceIdType.MESH)

    loads[0].wait()
    loads[1].wait()
    squares = jnp.zeros((trows, 1), f32)
    for i in range(2 * chunks):
        v = tokens[:, pl.ds(i * width, width)].astype(f32)
        squares += jnp.sum(v * v, axis=1, keepdims=True)
    scale = lax.rsqrt(squares / tokens.shape[1] + norm_eps)
    for ch in range(chunks):
        cols = pl.ds(pl.multiple_of(core * half + ch * width, 128), width)
        own[ch] = (tokens[:, cols].astype(f32) * scale * gain[:, cols]).astype(bf16)
    loads[2].wait()
    loads[3].wait()
    experts = chosen.shape[2]
    s_row = lax.broadcasted_iota(jnp.int32, (meta.shape[0], slots), 0)
    s_col = lax.broadcasted_iota(jnp.int32, (meta.shape[0], slots), 1)
    e_row = lax.broadcasted_iota(jnp.int32, (experts, meta.shape[1]), 0)
    e_lane = lax.broadcasted_iota(jnp.int32, (experts, meta.shape[1]), 1)
    table = jnp.zeros(meta.shape, f32)
    for i, (first, count) in enumerate(((0, low), (low, slots - low))):
        spread = jnp.where((s_row < count) & (s_col == s_row + first), 1.0, 0.0).astype(bf16)
        dead = lax.broadcasted_iota(jnp.int32, meta.shape, 0) >= count
        table += jnp.where(dead & (lane >= 2 * n * i) & (lane < 2 * n * i + n), float(trows), 0.0)
        for ref, shift in ((chosen, 0), (affinity, n)):
            place = jnp.where(e_lane == e_row + shift + 2 * n * i, 1.0, 0.0).astype(bf16)
            moved = dot(ref[:, 0, :].astype(f32).astype(bf16), place).astype(bf16)
            table += dot(spread, moved)
    meta[...] = table.astype(bf16)
    pl.semaphore_wait(barrier, len(peers))

    for ch in range(chunks):
        for g in range(2):
            hop(None, g, ch).start()
            if ch == 0:
                mhop(None, g).start()
    pk_own[0, pl.ds(UNIT, UNIT)] = jnp.zeros_like(pk_own[0, pl.ds(UNIT, UNIT)])
    own_hot = hot(meta[...].astype(f32), me, False)
    for ch in range(chunks):
        pk_own[0, pl.ds(0, UNIT), pl.ds(ch * width, width)] = dot(own_hot, own[ch]).astype(bf16)
    share(0).start()
    for load in loads[4:]:
        load.wait()

    def hidden_of(a, b):
        acc = dot(a, w_own[...]) + dot(b, w_oth[...])
        gate, upper = acc[:, :hid], acc[:, hid:]
        return (gate * jax.nn.sigmoid(gate) * upper).astype(bf16)

    def pick(t):
        for g in range(2):
            h = hot(mring[g, t - 1].astype(f32), me, False)
            for ch in range(chunks):
                pk_own[t, pl.ds(g * UNIT, UNIT), pl.ds(ch * width, width)] = dot(h, ring[g, t - 1, ch]).astype(bf16)
        share(t).start()

    def pick_far(h):
        for g in range(2):
            sides, ends = far_hot(mring[g, reach - 1].astype(f32), g, False)
            if far > 1:
                y = dot(sides[0], ring[g, reach - 1, 2 * h]) + dot(sides[1], ring[g, reach - 1, 2 * h + 1])
                far_out[g, h, pl.ds(0, far - 1)] = y.astype(bf16).reshape(far - 1, pack_rows, width)
            if h == 1:
                y = sum(dot(ends[ch], ring[g, reach - 1, ch]) for ch in range(chunks))
                far_out[g, 0, far - 1] = y.astype(bf16)
        first = [(far - 1, 0)] if far > 1 else []
        rest = [(far, 0)] + ([(far - 1, 1)] if far > 1 else [])
        rest += [(j, p) for j in range(far - 2, 0, -1) for p in (0, 1)]
        for j, p in rest if h else first:
            for g in range(2):
                far_send(g, j, p).start()

    def expert(b):
        share(b).wait_recv()
        h = hidden_of(pk_own[b], pk_oth[b])
        spot = lax.rem(b, 2)

        @pl.when(b >= 2)
        def _():
            give(ps.at[spot], b - 2).wait_send()

        ps[spot] = dot(h, d_oth[...]).astype(bf16)
        give(ps.at[spot], b).start()
        po[spot] = dot(h, d_own[...]).astype(bf16)

    def finish(b):
        give(ps.at[0], b).wait_recv()
        eo[b] = (po[lax.rem(b, 2)].astype(f32) + eo[b].astype(f32)).astype(bf16)

    def step(t, carry):
        @pl.when(t <= reach)
        def _():
            for g in range(2):
                mlanded(t - 1, g).wait_recv()

                @pl.when(t < reach)
                def _():
                    mhop(t - 1, g).start()

        for ch in range(chunks):
            @pl.when(t <= reach)
            def _():
                for g in range(2):
                    landed(t - 1, g, ch).wait_recv()

                    @pl.when(t < reach)
                    def _():
                        hop(t - 1, g, ch).start()

            if ch % 2:
                @pl.when(t == reach)
                def _():
                    pick_far(ch // 2)

            if ch == 0:
                @pl.when(t <= reach + 1)
                def _():
                    expert(t - 1)

            if ch == chunks - 2:
                @pl.when(t >= 2)
                def _():
                    finish(t - 2)

        @pl.when(t <= reach)
        def _():
            pick(t)

        return carry

    lax.fori_loop(1, reach + 3, step, 0)

    def far_arrive(js):
        for j in js:
            for g in range(2):
                for p in parts_of(j):
                    far_send(g, j, p).wait_recv()
            for g in range(2):
                for ch in range(chunks):
                    rows = dot_rows(packer(g, j == far, ch), far_got[g, part(j, ch), j - 1])
                    pk_own[reach + j, pl.ds(g * UNIT, UNIT), pl.ds(ch * width, width)] = rows.astype(bf16)
            share(reach + j).start()

    def far_experts(js):
        for j in js:
            share(reach + j).wait_recv()
        least, count = min(js), len(js)
        group, rows = pl.ds(reach + least, count), count * 2 * UNIT
        h = hidden_of(pk_own[group].reshape(rows, half), pk_oth[group].reshape(rows, half))
        spots = pl.ds(least - 1, count)
        psf[spots] = dot(h, d_oth[...]).astype(bf16).reshape(count, 2 * UNIT, half)
        for j in js:
            give(psf.at[j - 1], reach + j).start()
        pof[spots] = dot(h, d_own[...]).astype(bf16).reshape(count, 2 * UNIT, half)
        for j in js:
            b = reach + j
            give(psf.at[j - 1], b).wait_recv()
            eo[b] = (pof[j - 1].astype(f32) + eo[b].astype(f32)).astype(bf16)
            for g in range(2):
                for p in parts_of(j):
                    y = jnp.zeros((pack_rows, width), f32)
                    for ch in range(chunks):
                        if part(j, ch) == p:
                            y += dot(packer(g, j == far, ch), eo[b, pl.ds(g * UNIT, UNIT), pl.ds(ch * width, width)])
                    far_ret[g, p, j - 1] = y.astype(bf16)

    def far_return(js):
        for p in range(2):
            for j in js:
                if p in parts_of(j):
                    for g in range(2):
                        far_back(g, j, p).start()

    order = list(range(far, 0, -1))
    outer, inner = order[:2], order[2:]
    far_arrive(outer)
    far_experts(outer)
    far_arrive(inner)
    far_return(outer)
    if inner:
        far_experts(inner)
        far_return(inner)

    own_w = hot(meta[...].astype(f32), me, True)
    near_w = [hot(mring[g, reach - 1].astype(f32), me, True) for g in range(2)]
    far_w = [far_hot(mring[g, reach - 1].astype(f32), g, True) for g in range(2)]
    for h in range(2):
        for j in order:
            if h in parts_of(j):
                for g in range(2):
                    far_back(g, j, h).wait_recv()
        for ch in (2 * h, 2 * h + 1):
            cols = pl.ds(ch * width, width)
            for g in range(2):
                sides, ends = far_w[g]
                total = dot_rows(near_w[g], eo[reach, pl.ds(g * UNIT, UNIT), cols])
                total += dot_rows(ends[ch], far_in[g, 0, far - 1])
                if far > 1:
                    total += dot_rows(sides[ch % 2], far_in[g, h, pl.ds(0, far - 1)].reshape((far - 1) * pack_rows, width))
                top[g, ch] = total.astype(bf16)
                back(top.at[g, ch], reach - 1, g, ch).start()

    def fold(i, carry):
        d = reach - i
        hots = [hot(mring[g, d - 1].astype(f32), me, True) for g in range(2)]
        for ch in range(chunks):
            cols = pl.ds(ch * width, width)
            for g in range(2):
                add = dot_rows(hots[g], eo[d, pl.ds(g * UNIT, UNIT), cols])
                back(top.at[g, ch], d, g, ch).wait_recv()
                red[g, d, ch] = (red[g, d, ch].astype(f32) + add).astype(bf16)
                back(red.at[g, d, ch], d - 1, g, ch).start()
        return carry

    lax.fori_loop(1, reach, fold, 0)

    for ch in range(chunks):
        cols = pl.ds(ch * width, width)
        add = dot_rows(own_w, eo[0, pl.ds(0, UNIT), cols])
        for g in range(2):
            back(top.at[g, ch], 0, g, ch).wait_recv()
            add += red[g, 0, ch].astype(f32)
        out[:, cols] = add.astype(bf16)

    def drain(d, carry):
        for g in range(2):
            mlanded(d, g).wait_send()
            for ch in range(chunks):
                landed(d, g, ch).wait_send()
                back(top.at[g, ch], d, g, ch).wait_send()
        return carry

    lax.fori_loop(0, reach, drain, 0)

    def drain_share(d, carry):
        share(d).wait_send()
        return carry

    lax.fori_loop(0, batches, drain_share, 0)
    for b in (reach - 1, reach):
        give(ps.at[0], b).wait_send()
    for j in order:
        give(psf.at[j - 1], reach + j).wait_send()
        for g in range(2):
            for p in parts_of(j):
                far_send(g, j, p).wait_send()
                far_back(g, j, p).wait_send()


def shards(n, reach, chunks, tokens, norm_gain, gate_weight, up_weight, down_weight, chosen, affinity):
    trows, model = tokens.shape
    half = model // 2
    width = half // chunks
    slots = chosen.shape[2]
    hid = gate_weight.shape[2]
    far = n // 2 - reach
    pack_rows = up8(max(2 * slots, 4 * (slots - slots // 2)))
    chosen, affinity = [jnp.transpose(v, (2, 0, 1)) for v in (chosen, affinity)]
    lanes = max(128, 4 * n)
    dma, batches = pltpu.SemaphoreType.DMA, reach + far + 1
    vmem = pl.BlockSpec(memory_space=pltpu.VMEM)
    anywhere = pl.BlockSpec(memory_space=pl.ANY)
    return pl.pallas_call(
        functools.partial(kernel, n, reach, slots),
        out_shape=jax.ShapeDtypeStruct((trows, half), bf16),
        in_specs=[anywhere] * 7,
        out_specs=vmem,
        scratch_shapes=[
            pltpu.VMEM((trows, model), bf16),
            pltpu.VMEM((1, model), f32),
            pltpu.VMEM(chosen.shape, jnp.int32),
            pltpu.VMEM(chosen.shape, f32),
            pltpu.VMEM((UNIT // 2, lanes), bf16),
            pltpu.VMEM((chunks, trows, width), bf16),
            pltpu.VMEM((2, reach, chunks, trows, width), bf16),
            pltpu.VMEM((2, reach, UNIT // 2, lanes), bf16),
            pltpu.VMEM((half, 2 * hid), bf16),
            pltpu.VMEM((half, 2 * hid), bf16),
            pltpu.VMEM((hid, half), bf16),
            pltpu.VMEM((hid, half), bf16),
            pltpu.VMEM((batches, 2 * UNIT, half), bf16),
            pltpu.VMEM((batches, 2 * UNIT, half), bf16),
            pltpu.VMEM((batches, 2 * UNIT, half), bf16),
            pltpu.VMEM((2, 2 * UNIT, half), bf16),
            pltpu.VMEM((2, 2 * UNIT, half), bf16),
            pltpu.VMEM((far, 2 * UNIT, half), bf16),
            pltpu.VMEM((far, 2 * UNIT, half), bf16),
            pltpu.VMEM((2, 2, far, pack_rows, width), bf16),
            pltpu.VMEM((2, 2, far, pack_rows, width), bf16),
            pltpu.VMEM((2, 2, far, pack_rows, width), bf16),
            pltpu.VMEM((2, 2, far, pack_rows, width), bf16),
            pltpu.VMEM((2, reach, chunks, trows, width), bf16),
            pltpu.VMEM((2, chunks, trows, width), bf16),
            dma((10,)),
            dma((2, reach, chunks)), dma((2, reach, chunks)),
            dma((2, reach)), dma((2, reach)),
            dma((batches,)), dma((batches,)), dma((batches,)), dma((batches,)),
            dma((2, 2, far)), dma((2, 2, far)), dma((2, 2, far)), dma((2, 2, far)),
            dma((2, reach, chunks)), dma((2, reach, chunks)),
        ],
        compiler_params=pltpu.CompilerParams(
            collective_id=0, has_side_effects=True, vmem_limit_bytes=67043328
        ),
    )(tokens, norm_gain[None, :], chosen, affinity, gate_weight, up_weight, down_weight)


def solution(mesh):
    n = mesh.shape["ep"]
    in_specs = (
        P(("grp", "ep"), None),
        P(),
        P("ep", None, "tp"),
        P("ep", None, "tp"),
        P("ep", "tp", None),
        P(("grp", "ep"), None, None),
        P(("grp", "ep"), None, None),
    )
    body = functools.partial(shards, n, min(REACH, n // 2 - 1), CHUNKS)
    return jax.shard_map(body, mesh=mesh, in_specs=in_specs, out_specs=P(("grp", "ep"), "tp"), check_vma=False)
```

```python
import functools

import jax
import jax.numpy as jnp
from jax import lax
from jax.experimental import pallas as pl
from jax.experimental.pallas import tpu as pltpu
from jax.sharding import PartitionSpec as P

norm_eps = 1e-06
UNIT = 32
REACH = 10
CHUNKS = 4
f32, bf16 = jnp.float32, jnp.bfloat16


def up8(rows):
    return -(-rows // 8) * 8


def dot(a, b):
    return jnp.dot(a, b, preferred_element_type=f32)


def dot_rows(a, b):
    return lax.dot_general(a, b, (((0,), (0,)), ((), ())), preferred_element_type=f32)


def kernel(
    n, reach, slots, tokens_hbm, gain_hbm, chosen_hbm, affinity_hbm, gate_hbm, up_hbm, down_hbm, out,
    tokens, gain, chosen, affinity, meta, own, ring, mring, w_own, w_oth, d_own, d_oth,
    pk_own, pk_oth, eo, ps, po, psf, pof, far_out, far_got, far_ret, far_in, red, top,
    wsem, dsend, drecv, msend, mrecv, pxs, pxr, pas, par, fs, fr, gs, gr, rs, rr,
):
    me, core = lax.axis_index("ep"), lax.axis_index("tp")
    far = n // 2 - reach
    chunks, trows, width = own.shape
    half = chunks * width
    hid = w_own.shape[1] // 2
    pack_rows = far_out.shape[3]
    batches = reach + far + 1
    partner = {"tp": 1 - core}
    sign = (1, -1)

    def at(offset):
        return {"ep": lax.rem(me + offset + n, n)}

    def rcopy(src, dst, s, r, dev):
        return pltpu.make_async_remote_copy(
            src_ref=src, dst_ref=dst, send_sem=s, recv_sem=r, device_id=dev,
            device_id_type=pl.DeviceIdType.MESH,
        )

    def hop(d, g, ch):
        src = own.at[ch] if d is None else ring.at[g, d, ch]
        nxt = 0 if d is None else d + 1
        return rcopy(src, ring.at[g, nxt, ch], dsend.at[g, nxt, ch], drecv.at[g, nxt, ch], at(sign[g]))

    def landed(d, g, ch):
        return rcopy(own.at[ch], ring.at[g, d, ch], dsend.at[g, d, ch], drecv.at[g, d, ch], at(sign[g]))

    def mhop(d, g):
        src = meta if d is None else mring.at[g, d]
        nxt = 0 if d is None else d + 1
        return rcopy(src, mring.at[g, nxt], msend.at[g, nxt], mrecv.at[g, nxt], at(sign[g]))

    def mlanded(d, g):
        return rcopy(meta, mring.at[g, d], msend.at[g, d], mrecv.at[g, d], at(sign[g]))

    def share(d):
        return rcopy(pk_own.at[d], pk_oth.at[d], pxs.at[d], pxr.at[d], partner)

    def give(src, d):
        return rcopy(src, eo.at[d], pas.at[d], par.at[d], partner)

    def far_copy(src, dst, s, r, g, j, h, way):
        return rcopy(
            src.at[g, h, j - 1], dst.at[g, h, j - 1], s.at[g, h, j - 1], r.at[g, h, j - 1], at(way * sign[g] * j)
        )

    def far_send(g, j, h):
        return far_copy(far_out, far_got, fs, fr, g, j, h, 1)

    def far_back(g, j, h):
        return far_copy(far_ret, far_in, gs, gr, g, j, h, -1)

    def parts_of(j):
        return (0,) if j == far else (0, 1)

    def back(src, d, g, ch):
        return rcopy(src, red.at[g, d, ch], rs.at[g, d, ch], rr.at[g, d, ch], at(-sign[g]))

    low = slots // 2
    lane = lax.broadcasted_iota(jnp.int32, meta.shape, 1)
    tok = lax.broadcasted_iota(jnp.int32, (UNIT, trows), 1).astype(f32)

    def column(m, index):
        pair = [jnp.sum(jnp.where(lane == index + 2 * n * i, m, 0.0), axis=1, keepdims=True) for i in range(2)]
        return jnp.concatenate(pair, axis=0)

    def hot(m, e, weighted):
        value = column(m, n + e) if weighted else 1.0
        return jnp.where(column(m, e) == tok, value, 0.0).astype(bf16)

    pack_r = lax.broadcasted_iota(jnp.int32, (pack_rows, UNIT), 0)
    pack_s = lax.broadcasted_iota(jnp.int32, (pack_rows, UNIT), 1)

    def packer(g, end, ch):
        count, first, place = slots, 0, ch % 2
        if end:
            count, first, place = (low, 0, ch) if g == 0 else (slots - low, low, ch)
        local = pack_r - place * count
        wanted = local + first
        wanted = jnp.where(wanted < low, wanted, wanted - low + UNIT // 2)
        keep = (local >= 0) & (local < count) & (pack_s == wanted)
        return jnp.where(keep, 1.0, 0.0).astype(bf16)

    def part(j, ch):
        return 0 if j == far else ch // 2

    def far_hot(m, g, weighted):
        hots = [hot(m, lax.rem(me + sign[g] * j + n, n), weighted) for j in range(1, far + 1)]
        sides = []
        for ch in range(2 if far > 1 else 0):
            pk = packer(g, False, ch)
            sides.append(jnp.concatenate([dot(pk, h) for h in hots[:-1]], axis=0).astype(bf16))
        ends = [dot(packer(g, True, ch), hots[-1]).astype(bf16) for ch in range(chunks)]
        return sides, ends

    loads = []
    for i, (src, dst) in enumerate((
        (tokens_hbm, tokens),
        (gain_hbm, gain),
        (chosen_hbm, chosen),
        (affinity_hbm, affinity),
        (gate_hbm.at[0, pl.ds(core * half, half)], w_own.at[:, pl.ds(0, hid)]),
        (up_hbm.at[0, pl.ds(core * half, half)], w_own.at[:, pl.ds(hid, hid)]),
        (gate_hbm.at[0, pl.ds((1 - core) * half, half)], w_oth.at[:, pl.ds(0, hid)]),
        (up_hbm.at[0, pl.ds((1 - core) * half, half)], w_oth.at[:, pl.ds(hid, hid)]),
        (down_hbm.at[0, :, pl.ds(pl.multiple_of(core * half, 128), half)], d_own),
        (down_hbm.at[0, :, pl.ds(pl.multiple_of((1 - core) * half, 128), half)], d_oth),
    )):
        loads.append(pltpu.make_async_copy(src, dst, wsem.at[i]))
        loads[-1].start()

    barrier = pltpu.get_barrier_semaphore()
    peers = [at(1), at(-1), partner]
    for peer in peers:
        pl.semaphore_signal(barrier, inc=1, device_id=peer, device_id_type=pl.DeviceIdType.MESH)

    loads[0].wait()
    loads[1].wait()
    squares = jnp.zeros((trows, 1), f32)
    for i in range(2 * chunks):
        v = tokens[:, pl.ds(i * width, width)].astype(f32)
        squares += jnp.sum(v * v, axis=1, keepdims=True)
    scale = lax.rsqrt(squares / tokens.shape[1] + norm_eps)
    for ch in range(chunks):
        cols = pl.ds(pl.multiple_of(core * half + ch * width, 128), width)
        own[ch] = (tokens[:, cols].astype(f32) * scale * gain[:, cols]).astype(bf16)
    loads[2].wait()
    loads[3].wait()
    experts = chosen.shape[2]
    s_row = lax.broadcasted_iota(jnp.int32, (meta.shape[0], slots), 0)
    s_col = lax.broadcasted_iota(jnp.int32, (meta.shape[0], slots), 1)
    e_row = lax.broadcasted_iota(jnp.int32, (experts, meta.shape[1]), 0)
    e_lane = lax.broadcasted_iota(jnp.int32, (experts, meta.shape[1]), 1)
    table = jnp.zeros(meta.shape, f32)
    for i, (first, count) in enumerate(((0, low), (low, slots - low))):
        spread = jnp.where((s_row < count) & (s_col == s_row + first), 1.0, 0.0).astype(bf16)
        dead = lax.broadcasted_iota(jnp.int32, meta.shape, 0) >= count
        table += jnp.where(dead & (lane >= 2 * n * i) & (lane < 2 * n * i + n), float(trows), 0.0)
        for ref, shift in ((chosen, 0), (affinity, n)):
            place = jnp.where(e_lane == e_row + shift + 2 * n * i, 1.0, 0.0).astype(bf16)
            moved = dot(ref[:, 0, :].astype(f32).astype(bf16), place).astype(bf16)
            table += dot(spread, moved)
    meta[...] = table.astype(bf16)
    pl.semaphore_wait(barrier, len(peers))

    for ch in range(chunks):
        for g in range(2):
            hop(None, g, ch).start()
            if ch == 0:
                mhop(None, g).start()
    pk_own[0, pl.ds(UNIT, UNIT)] = jnp.zeros_like(pk_own[0, pl.ds(UNIT, UNIT)])
    own_hot = hot(meta[...].astype(f32), me, False)
    for ch in range(chunks):
        pk_own[0, pl.ds(0, UNIT), pl.ds(ch * width, width)] = dot(own_hot, own[ch]).astype(bf16)
    share(0).start()
    for load in loads[4:]:
        load.wait()

    def hidden_of(a, b):
        acc = dot(a, w_own[...]) + dot(b, w_oth[...])
        gate, upper = acc[:, :hid], acc[:, hid:]
        return (gate * jax.nn.sigmoid(gate) * upper).astype(bf16)

    def pick(t):
        for g in range(2):
            h = hot(mring[g, t - 1].astype(f32), me, False)
            for ch in range(chunks):
                pk_own[t, pl.ds(g * UNIT, UNIT), pl.ds(ch * width, width)] = dot(h, ring[g, t - 1, ch]).astype(bf16)
        share(t).start()

    def pick_far(h):
        for g in range(2):
            sides, ends = far_hot(mring[g, reach - 1].astype(f32), g, False)
            if far > 1:
                y = dot(sides[0], ring[g, reach - 1, 2 * h]) + dot(sides[1], ring[g, reach - 1, 2 * h + 1])
                far_out[g, h, pl.ds(0, far - 1)] = y.astype(bf16).reshape(far - 1, pack_rows, width)
            if h == 1:
                y = sum(dot(ends[ch], ring[g, reach - 1, ch]) for ch in range(chunks))
                far_out[g, 0, far - 1] = y.astype(bf16)
        first = [(far - 1, 0)] if far > 1 else []
        rest = [(far, 0)] + ([(far - 1, 1)] if far > 1 else [])
        rest += [(j, p) for j in range(far - 2, 0, -1) for p in (0, 1)]
        for j, p in rest if h else first:
            for g in range(2):
                far_send(g, j, p).start()

    def expert(b):
        share(b).wait_recv()
        h = hidden_of(pk_own[b], pk_oth[b])
        spot = lax.rem(b, 2)

        @pl.when(b >= 2)
        def _():
            give(ps.at[spot], b - 2).wait_send()

        ps[spot] = dot(h, d_oth[...]).astype(bf16)
        give(ps.at[spot], b).start()
        po[spot] = dot(h, d_own[...]).astype(bf16)

    def finish(b):
        give(ps.at[0], b).wait_recv()
        eo[b] = (po[lax.rem(b, 2)].astype(f32) + eo[b].astype(f32)).astype(bf16)

    def step(t, carry):
        @pl.when(t <= reach)
        def _():
            for g in range(2):
                mlanded(t - 1, g).wait_recv()

                @pl.when(t < reach)
                def _():
                    mhop(t - 1, g).start()

        for ch in range(chunks):
            @pl.when(t <= reach)
            def _():
                for g in range(2):
                    landed(t - 1, g, ch).wait_recv()

                    @pl.when(t < reach)
                    def _():
                        hop(t - 1, g, ch).start()

            if ch % 2:
                @pl.when(t == reach)
                def _():
                    pick_far(ch // 2)

            if ch == 0:
                @pl.when(t <= reach + 1)
                def _():
                    expert(t - 1)

            if ch == chunks - 2:
                @pl.when(t >= 2)
                def _():
                    finish(t - 2)

        @pl.when(t <= reach)
        def _():
            pick(t)

        return carry

    lax.fori_loop(1, reach + 3, step, 0)

    def far_arrive(js):
        for j in js:
            for g in range(2):
                for p in parts_of(j):
                    far_send(g, j, p).wait_recv()
            for g in range(2):
                for ch in range(chunks):
                    rows = dot_rows(packer(g, j == far, ch), far_got[g, part(j, ch), j - 1])
                    pk_own[reach + j, pl.ds(g * UNIT, UNIT), pl.ds(ch * width, width)] = rows.astype(bf16)
            share(reach + j).start()

    def far_experts(js):
        for j in js:
            share(reach + j).wait_recv()
        least, count = min(js), len(js)
        group, rows = pl.ds(reach + least, count), count * 2 * UNIT
        h = hidden_of(pk_own[group].reshape(rows, half), pk_oth[group].reshape(rows, half))
        spots = pl.ds(least - 1, count)
        psf[spots] = dot(h, d_oth[...]).astype(bf16).reshape(count, 2 * UNIT, half)
        for j in js:
            give(psf.at[j - 1], reach + j).start()
        pof[spots] = dot(h, d_own[...]).astype(bf16).reshape(count, 2 * UNIT, half)
        for j in js:
            b = reach + j
            give(psf.at[j - 1], b).wait_recv()
            eo[b] = (pof[j - 1].astype(f32) + eo[b].astype(f32)).astype(bf16)
            for g in range(2):
                for p in parts_of(j):
                    y = jnp.zeros((pack_rows, width), f32)
                    for ch in range(chunks):
                        if part(j, ch) == p:
                            y += dot(packer(g, j == far, ch), eo[b, pl.ds(g * UNIT, UNIT), pl.ds(ch * width, width)])
                    far_ret[g, p, j - 1] = y.astype(bf16)

    def far_return(js):
        for p in range(2):
            for j in js:
                if p in parts_of(j):
                    for g in range(2):
                        far_back(g, j, p).start()

    order = list(range(far, 0, -1))
    outer, inner = order[:2], order[2:]
    far_arrive(outer)
    far_experts(outer)
    early = inner[:max(len(inner) - 2, 0)]
    far_arrive(early)
    far_return(outer[:1])
    far_arrive(inner[len(early):])
    far_return(outer[1:])
    if inner:
        far_experts(inner)
        far_return(inner)

    own_w = hot(meta[...].astype(f32), me, True)
    near_w = [hot(mring[g, reach - 1].astype(f32), me, True) for g in range(2)]
    far_w = [far_hot(mring[g, reach - 1].astype(f32), g, True) for g in range(2)]
    for h in range(2):
        for j in order:
            if h in parts_of(j):
                for g in range(2):
                    far_back(g, j, h).wait_recv()
        for ch in (2 * h, 2 * h + 1):
            cols = pl.ds(ch * width, width)
            for g in range(2):
                sides, ends = far_w[g]
                total = dot_rows(near_w[g], eo[reach, pl.ds(g * UNIT, UNIT), cols])
                total += dot_rows(ends[ch], far_in[g, 0, far - 1])
                if far > 1:
                    total += dot_rows(sides[ch % 2], far_in[g, h, pl.ds(0, far - 1)].reshape((far - 1) * pack_rows, width))
                top[g, ch] = total.astype(bf16)
                back(top.at[g, ch], reach - 1, g, ch).start()

    def fold(i, carry):
        d = reach - i
        hots = [hot(mring[g, d - 1].astype(f32), me, True) for g in range(2)]
        for ch in range(chunks):
            cols = pl.ds(ch * width, width)
            for g in range(2):
                add = dot_rows(hots[g], eo[d, pl.ds(g * UNIT, UNIT), cols])
                back(top.at[g, ch], d, g, ch).wait_recv()
                red[g, d, ch] = (red[g, d, ch].astype(f32) + add).astype(bf16)
                back(red.at[g, d, ch], d - 1, g, ch).start()
        return carry

    lax.fori_loop(1, reach, fold, 0)

    for ch in range(chunks):
        cols = pl.ds(ch * width, width)
        add = dot_rows(own_w, eo[0, pl.ds(0, UNIT), cols])
        for g in range(2):
            back(top.at[g, ch], 0, g, ch).wait_recv()
            add += red[g, 0, ch].astype(f32)
        out[:, cols] = add.astype(bf16)

    def drain(d, carry):
        for g in range(2):
            mlanded(d, g).wait_send()
            for ch in range(chunks):
                landed(d, g, ch).wait_send()
                back(top.at[g, ch], d, g, ch).wait_send()
        return carry

    lax.fori_loop(0, reach, drain, 0)

    def drain_share(d, carry):
        share(d).wait_send()
        return carry

    lax.fori_loop(0, batches, drain_share, 0)
    for b in (reach - 1, reach):
        give(ps.at[0], b).wait_send()
    for j in order:
        give(psf.at[j - 1], reach + j).wait_send()
        for g in range(2):
            for p in parts_of(j):
                far_send(g, j, p).wait_send()
                far_back(g, j, p).wait_send()


def shards(n, reach, chunks, tokens, norm_gain, gate_weight, up_weight, down_weight, chosen, affinity):
    trows, model = tokens.shape
    half = model // 2
    width = half // chunks
    slots = chosen.shape[2]
    hid = gate_weight.shape[2]
    far = n // 2 - reach
    pack_rows = up8(max(2 * slots, 4 * (slots - slots // 2)))
    chosen, affinity = [jnp.transpose(v, (2, 0, 1)) for v in (chosen, affinity)]
    lanes = max(128, 4 * n)
    dma, batches = pltpu.SemaphoreType.DMA, reach + far + 1
    vmem = pl.BlockSpec(memory_space=pltpu.VMEM)
    anywhere = pl.BlockSpec(memory_space=pl.ANY)
    return pl.pallas_call(
        functools.partial(kernel, n, reach, slots),
        out_shape=pltpu.VMEM((trows, half), bf16),
        in_specs=[anywhere] * 7,
        out_specs=vmem,
        scratch_shapes=[
            pltpu.VMEM((trows, model), bf16),
            pltpu.VMEM((1, model), f32),
            pltpu.VMEM(chosen.shape, jnp.int32),
            pltpu.VMEM(chosen.shape, f32),
            pltpu.VMEM((UNIT // 2, lanes), bf16),
            pltpu.VMEM((chunks, trows, width), bf16),
            pltpu.VMEM((2, reach, chunks, trows, width), bf16),
            pltpu.VMEM((2, reach, UNIT // 2, lanes), bf16),
            pltpu.VMEM((half, 2 * hid), bf16),
            pltpu.VMEM((half, 2 * hid), bf16),
            pltpu.VMEM((hid, half), bf16),
            pltpu.VMEM((hid, half), bf16),
            pltpu.VMEM((batches, 2 * UNIT, half), bf16),
            pltpu.VMEM((batches, 2 * UNIT, half), bf16),
            pltpu.VMEM((batches, 2 * UNIT, half), bf16),
            pltpu.VMEM((2, 2 * UNIT, half), bf16),
            pltpu.VMEM((2, 2 * UNIT, half), bf16),
            pltpu.VMEM((far, 2 * UNIT, half), bf16),
            pltpu.VMEM((far, 2 * UNIT, half), bf16),
            pltpu.VMEM((2, 2, far, pack_rows, width), bf16),
            pltpu.VMEM((2, 2, far, pack_rows, width), bf16),
            pltpu.VMEM((2, 2, far, pack_rows, width), bf16),
            pltpu.VMEM((2, 2, far, pack_rows, width), bf16),
            pltpu.VMEM((2, reach, chunks, trows, width), bf16),
            pltpu.VMEM((2, chunks, trows, width), bf16),
            dma((10,)),
            dma((2, reach, chunks)), dma((2, reach, chunks)),
            dma((2, reach)), dma((2, reach)),
            dma((batches,)), dma((batches,)), dma((batches,)), dma((batches,)),
            dma((2, 2, far)), dma((2, 2, far)), dma((2, 2, far)), dma((2, 2, far)),
            dma((2, reach, chunks)), dma((2, reach, chunks)),
        ],
        compiler_params=pltpu.CompilerParams(
            collective_id=0, has_side_effects=True, vmem_limit_bytes=58 * 2**20
        ),
    )(tokens, norm_gain[None, :], chosen, affinity, gate_weight, up_weight, down_weight)


def solution(mesh):
    n = mesh.shape["ep"]
    in_specs = (
        P(("grp", "ep"), None),
        P(),
        P("ep", None, "tp"),
        P("ep", None, "tp"),
        P("ep", "tp", None),
        P(("grp", "ep"), None, None),
        P(("grp", "ep"), None, None),
    )
    body = functools.partial(shards, n, min(REACH, n // 2 - 1), CHUNKS)
    return jax.shard_map(body, mesh=mesh, in_specs=in_specs, out_specs=P(("grp", "ep"), "tp"), check_vma=False)
```

```python
import functools

import jax
import jax.numpy as jnp
from jax import lax
from jax.experimental import pallas as pl
from jax.experimental.pallas import tpu as pltpu
from jax.sharding import PartitionSpec as P

norm_eps = 1e-06
UNIT = 32
REACH = 10
CHUNKS = 4
f32, bf16 = jnp.float32, jnp.bfloat16


def up8(rows):
    return -(-rows // 8) * 8


def dot(a, b):
    return jnp.dot(a, b, preferred_element_type=f32)


def dot_rows(a, b):
    return lax.dot_general(a, b, (((0,), (0,)), ((), ())), preferred_element_type=f32)


def kernel(
    n, reach, slots, tokens_hbm, gain_hbm, chosen_hbm, affinity_hbm, gate_hbm, up_hbm, down_hbm, out,
    tokens, gain, chosen, affinity, meta, own, ring, mring, w_own, w_oth, d_own, d_oth,
    pk_own, pk_oth, eo, ps, po, psf, pof, far_out, far_got, far_ret, far_in, red, top,
    wsem, dsend, drecv, msend, mrecv, pxs, pxr, pas, par, fs, fr, gs, gr, rs, rr,
):
    me, core = lax.axis_index("ep"), lax.axis_index("tp")
    far = n // 2 - reach
    chunks, trows, width = own.shape
    half = chunks * width
    hid = w_own.shape[1] // 2
    pack_rows = far_out.shape[3]
    batches = reach + far + 1
    partner = {"tp": 1 - core}
    sign = (1, -1)

    def at(offset):
        return {"ep": lax.rem(me + offset + n, n)}

    def rcopy(src, dst, s, r, dev):
        return pltpu.make_async_remote_copy(
            src_ref=src, dst_ref=dst, send_sem=s, recv_sem=r, device_id=dev,
            device_id_type=pl.DeviceIdType.MESH,
        )

    def hop(d, g, ch):
        src = own.at[ch] if d is None else ring.at[g, d, ch]
        nxt = 0 if d is None else d + 1
        return rcopy(src, ring.at[g, nxt, ch], dsend.at[g, nxt, ch], drecv.at[g, nxt, ch], at(sign[g]))

    def landed(d, g, ch):
        return rcopy(own.at[ch], ring.at[g, d, ch], dsend.at[g, d, ch], drecv.at[g, d, ch], at(sign[g]))

    def mhop(d, g):
        src = meta if d is None else mring.at[g, d]
        nxt = 0 if d is None else d + 1
        return rcopy(src, mring.at[g, nxt], msend.at[g, nxt], mrecv.at[g, nxt], at(sign[g]))

    def mlanded(d, g):
        return rcopy(meta, mring.at[g, d], msend.at[g, d], mrecv.at[g, d], at(sign[g]))

    def share(d):
        return rcopy(pk_own.at[d], pk_oth.at[d], pxs.at[d], pxr.at[d], partner)

    def give(src, d):
        return rcopy(src, eo.at[d], pas.at[d], par.at[d], partner)

    def far_copy(src, dst, s, r, g, j, h, way):
        return rcopy(
            src.at[g, h, j - 1], dst.at[g, h, j - 1], s.at[g, h, j - 1], r.at[g, h, j - 1], at(way * sign[g] * j)
        )

    def far_send(g, j, h):
        return far_copy(far_out, far_got, fs, fr, g, j, h, 1)

    def far_back(g, j, h):
        return far_copy(far_ret, far_in, gs, gr, g, j, h, -1)

    def parts_of(j):
        return (0,) if j == far else (0, 1)

    def back(src, d, g, ch):
        return rcopy(src, red.at[g, d, ch], rs.at[g, d, ch], rr.at[g, d, ch], at(-sign[g]))

    low = slots // 2
    lane = lax.broadcasted_iota(jnp.int32, meta.shape, 1)
    tok = lax.broadcasted_iota(jnp.int32, (UNIT, trows), 1).astype(f32)

    def column(m, index):
        pair = [jnp.sum(jnp.where(lane == index + 2 * n * i, m, 0.0), axis=1, keepdims=True) for i in range(2)]
        return jnp.concatenate(pair, axis=0)

    def hot(m, e, weighted):
        value = column(m, n + e) if weighted else 1.0
        return jnp.where(column(m, e) == tok, value, 0.0).astype(bf16)

    pack_r = lax.broadcasted_iota(jnp.int32, (pack_rows, UNIT), 0)
    pack_s = lax.broadcasted_iota(jnp.int32, (pack_rows, UNIT), 1)

    def packer(g, end, ch):
        count, first, place = slots, 0, ch % 2
        if end:
            count, first, place = (low, 0, ch) if g == 0 else (slots - low, low, ch)
        local = pack_r - place * count
        wanted = local + first
        wanted = jnp.where(wanted < low, wanted, wanted - low + UNIT // 2)
        keep = (local >= 0) & (local < count) & (pack_s == wanted)
        return jnp.where(keep, 1.0, 0.0).astype(bf16)

    def part(j, ch):
        return 0 if j == far else ch // 2

    def far_hot(m, g, weighted):
        hots = [hot(m, lax.rem(me + sign[g] * j + n, n), weighted) for j in range(1, far + 1)]
        sides = []
        for ch in range(2 if far > 1 else 0):
            pk = packer(g, False, ch)
            sides.append(jnp.concatenate([dot(pk, h) for h in hots[:-1]], axis=0).astype(bf16))
        ends = [dot(packer(g, True, ch), hots[-1]).astype(bf16) for ch in range(chunks)]
        return sides, ends

    barrier = pltpu.get_barrier_semaphore()
    peers = [at(1), at(-1), partner]
    for peer in peers:
        pl.semaphore_signal(barrier, inc=1, device_id=peer, device_id_type=pl.DeviceIdType.MESH)

    loads = []
    for i, (src, dst) in enumerate((
        (tokens_hbm, tokens),
        (gain_hbm, gain),
        (chosen_hbm, chosen),
        (affinity_hbm, affinity),
        (gate_hbm.at[0, pl.ds(core * half, half)], w_own.at[:, pl.ds(0, hid)]),
        (up_hbm.at[0, pl.ds(core * half, half)], w_own.at[:, pl.ds(hid, hid)]),
        (gate_hbm.at[0, pl.ds((1 - core) * half, half)], w_oth.at[:, pl.ds(0, hid)]),
        (up_hbm.at[0, pl.ds((1 - core) * half, half)], w_oth.at[:, pl.ds(hid, hid)]),
        (down_hbm.at[0, :, pl.ds(pl.multiple_of(core * half, 128), half)], d_own),
        (down_hbm.at[0, :, pl.ds(pl.multiple_of((1 - core) * half, 128), half)], d_oth),
    )):
        loads.append(pltpu.make_async_copy(src, dst, wsem.at[i]))
        loads[-1].start()

    loads[0].wait()
    loads[1].wait()
    squares = jnp.zeros((trows, 1), f32)
    for i in range(2 * chunks):
        v = tokens[:, pl.ds(i * width, width)].astype(f32)
        squares += jnp.sum(v * v, axis=1, keepdims=True)
    scale = lax.rsqrt(squares / tokens.shape[1] + norm_eps)
    for ch in range(chunks):
        cols = pl.ds(pl.multiple_of(core * half + ch * width, 128), width)
        own[ch] = (tokens[:, cols].astype(f32) * scale * gain[:, cols]).astype(bf16)
    loads[2].wait()
    loads[3].wait()
    experts = chosen.shape[2]
    s_row = lax.broadcasted_iota(jnp.int32, (meta.shape[0], slots), 0)
    s_col = lax.broadcasted_iota(jnp.int32, (meta.shape[0], slots), 1)
    e_row = lax.broadcasted_iota(jnp.int32, (experts, meta.shape[1]), 0)
    e_lane = lax.broadcasted_iota(jnp.int32, (experts, meta.shape[1]), 1)
    table = jnp.zeros(meta.shape, f32)
    for i, (first, count) in enumerate(((0, low), (low, slots - low))):
        spread = jnp.where((s_row < count) & (s_col == s_row + first), 1.0, 0.0).astype(bf16)
        dead = lax.broadcasted_iota(jnp.int32, meta.shape, 0) >= count
        table += jnp.where(dead & (lane >= 2 * n * i) & (lane < 2 * n * i + n), float(trows), 0.0)
        for ref, shift in ((chosen, 0), (affinity, n)):
            place = jnp.where(e_lane == e_row + shift + 2 * n * i, 1.0, 0.0).astype(bf16)
            moved = dot(ref[:, 0, :].astype(f32).astype(bf16), place).astype(bf16)
            table += dot(spread, moved)
    meta[...] = table.astype(bf16)
    pl.semaphore_wait(barrier, len(peers))

    for ch in range(chunks):
        for g in range(2):
            hop(None, g, ch).start()
            if ch == 0:
                mhop(None, g).start()
    pk_own[0, pl.ds(UNIT, UNIT)] = jnp.zeros_like(pk_own[0, pl.ds(UNIT, UNIT)])
    own_hot = hot(meta[...].astype(f32), me, False)
    for ch in range(chunks):
        pk_own[0, pl.ds(0, UNIT), pl.ds(ch * width, width)] = dot(own_hot, own[ch]).astype(bf16)
    share(0).start()
    for load in loads[4:]:
        load.wait()

    def hidden_of(a, b):
        acc = dot(a, w_own[...]) + dot(b, w_oth[...])
        gate, upper = acc[:, :hid], acc[:, hid:]
        return (gate * jax.nn.sigmoid(gate) * upper).astype(bf16)

    def pick(t):
        for g in range(2):
            h = hot(mring[g, t - 1].astype(f32), me, False)
            for ch in range(chunks):
                pk_own[t, pl.ds(g * UNIT, UNIT), pl.ds(ch * width, width)] = dot(h, ring[g, t - 1, ch]).astype(bf16)
        share(t).start()

    def pick_far(h):
        for g in range(2):
            sides, ends = far_hot(mring[g, reach - 1].astype(f32), g, False)
            if far > 1:
                y = dot(sides[0], ring[g, reach - 1, 2 * h]) + dot(sides[1], ring[g, reach - 1, 2 * h + 1])
                far_out[g, h, pl.ds(0, far - 1)] = y.astype(bf16).reshape(far - 1, pack_rows, width)
            if h == 1:
                y = sum(dot(ends[ch], ring[g, reach - 1, ch]) for ch in range(chunks))
                far_out[g, 0, far - 1] = y.astype(bf16)
        first = [(far - 1, 0)] if far > 1 else []
        rest = [(far, 0)] + ([(far - 1, 1)] if far > 1 else [])
        rest += [(j, p) for j in range(far - 2, 0, -1) for p in (0, 1)]
        for j, p in rest if h else first:
            for g in range(2):
                far_send(g, j, p).start()

    def expert(b):
        share(b).wait_recv()
        h = hidden_of(pk_own[b], pk_oth[b])
        spot = lax.rem(b, 2)

        @pl.when(b >= 2)
        def _():
            give(ps.at[spot], b - 2).wait_send()

        ps[spot] = dot(h, d_oth[...]).astype(bf16)
        give(ps.at[spot], b).start()
        po[spot] = dot(h, d_own[...]).astype(bf16)

    def finish(b):
        give(ps.at[0], b).wait_recv()
        eo[b] = (po[lax.rem(b, 2)].astype(f32) + eo[b].astype(f32)).astype(bf16)

    def step(t, carry):
        @pl.when(t <= reach)
        def _():
            for g in range(2):
                mlanded(t - 1, g).wait_recv()

                @pl.when(t < reach)
                def _():
                    mhop(t - 1, g).start()

        for ch in range(chunks):
            @pl.when(t <= reach)
            def _():
                for g in range(2):
                    landed(t - 1, g, ch).wait_recv()

                    @pl.when(t < reach)
                    def _():
                        hop(t - 1, g, ch).start()

            if ch % 2:
                @pl.when(t == reach)
                def _():
                    pick_far(ch // 2)

            if ch == 0:
                @pl.when(t <= reach + 1)
                def _():
                    expert(t - 1)

            if ch == chunks - 2:
                @pl.when(t >= 2)
                def _():
                    finish(t - 2)

        @pl.when(t <= reach)
        def _():
            pick(t)

        return carry

    lax.fori_loop(1, reach + 3, step, 0)

    def far_arrive(js):
        for j in js:
            for g in range(2):
                for p in parts_of(j):
                    far_send(g, j, p).wait_recv()
            for g in range(2):
                for ch in range(chunks):
                    rows = dot_rows(packer(g, j == far, ch), far_got[g, part(j, ch), j - 1])
                    pk_own[reach + j, pl.ds(g * UNIT, UNIT), pl.ds(ch * width, width)] = rows.astype(bf16)
            share(reach + j).start()

    def far_experts(js):
        for j in js:
            share(reach + j).wait_recv()
        least, count = min(js), len(js)
        group, rows = pl.ds(reach + least, count), count * 2 * UNIT
        h = hidden_of(pk_own[group].reshape(rows, half), pk_oth[group].reshape(rows, half))
        spots = pl.ds(least - 1, count)
        psf[spots] = dot(h, d_oth[...]).astype(bf16).reshape(count, 2 * UNIT, half)
        for j in js:
            give(psf.at[j - 1], reach + j).start()
        pof[spots] = dot(h, d_own[...]).astype(bf16).reshape(count, 2 * UNIT, half)
        for j in js:
            b = reach + j
            give(psf.at[j - 1], b).wait_recv()
            eo[b] = (pof[j - 1].astype(f32) + eo[b].astype(f32)).astype(bf16)
            for g in range(2):
                for p in parts_of(j):
                    y = jnp.zeros((pack_rows, width), f32)
                    for ch in range(chunks):
                        if part(j, ch) == p:
                            y += dot(packer(g, j == far, ch), eo[b, pl.ds(g * UNIT, UNIT), pl.ds(ch * width, width)])
                    far_ret[g, p, j - 1] = y.astype(bf16)

    def far_return(js, p):
        for j in js:
            if p in parts_of(j):
                for g in range(2):
                    far_back(g, j, p).start()

    order = list(range(far, 0, -1))
    groups = [order[:2], order[2:-2], order[-2:]] if far > 4 else [order]
    for i, js in enumerate(groups):
        far_arrive(js)
        far_experts(js)
        far_return(js, 0)
        if i < len(groups) - 2:
            far_return(js, 1)
    for js in groups[-2:]:
        far_return(js, 1)

    own_w = hot(meta[...].astype(f32), me, True)
    near_w = [hot(mring[g, reach - 1].astype(f32), me, True) for g in range(2)]
    far_w = [far_hot(mring[g, reach - 1].astype(f32), g, True) for g in range(2)]
    for h in range(2):
        for j in order:
            if h in parts_of(j):
                for g in range(2):
                    far_back(g, j, h).wait_recv()
        for ch in (2 * h, 2 * h + 1):
            cols = pl.ds(ch * width, width)
            for g in range(2):
                sides, ends = far_w[g]
                total = dot_rows(near_w[g], eo[reach, pl.ds(g * UNIT, UNIT), cols])
                total += dot_rows(ends[ch], far_in[g, 0, far - 1])
                if far > 1:
                    total += dot_rows(sides[ch % 2], far_in[g, h, pl.ds(0, far - 1)].reshape((far - 1) * pack_rows, width))
                top[g, ch] = total.astype(bf16)
                back(top.at[g, ch], reach - 1, g, ch).start()

    def fold(i, carry):
        d = reach - i
        hots = [hot(mring[g, d - 1].astype(f32), me, True) for g in range(2)]
        for ch in range(chunks):
            cols = pl.ds(ch * width, width)
            for g in range(2):
                add = dot_rows(hots[g], eo[d, pl.ds(g * UNIT, UNIT), cols])
                back(top.at[g, ch], d, g, ch).wait_recv()
                red[g, d, ch] = (red[g, d, ch].astype(f32) + add).astype(bf16)
                back(red.at[g, d, ch], d - 1, g, ch).start()
        return carry

    lax.fori_loop(1, reach, fold, 0)

    for ch in range(chunks):
        cols = pl.ds(ch * width, width)
        add = dot_rows(own_w, eo[0, pl.ds(0, UNIT), cols])
        for g in range(2):
            back(top.at[g, ch], 0, g, ch).wait_recv()
            add += red[g, 0, ch].astype(f32)
        out[:, cols] = add.astype(bf16)

    def drain(d, carry):
        for g in range(2):
            mlanded(d, g).wait_send()
            for ch in range(chunks):
                landed(d, g, ch).wait_send()
                back(top.at[g, ch], d, g, ch).wait_send()
        return carry

    lax.fori_loop(0, reach, drain, 0)

    def drain_share(d, carry):
        share(d).wait_send()
        return carry

    lax.fori_loop(0, batches, drain_share, 0)
    for b in (reach - 1, reach):
        give(ps.at[0], b).wait_send()
    for j in order:
        give(psf.at[j - 1], reach + j).wait_send()
        for g in range(2):
            for p in parts_of(j):
                far_send(g, j, p).wait_send()
                far_back(g, j, p).wait_send()


def shards(n, reach, chunks, tokens, norm_gain, gate_weight, up_weight, down_weight, chosen, affinity):
    trows, model = tokens.shape
    half = model // 2
    width = half // chunks
    slots = chosen.shape[2]
    hid = gate_weight.shape[2]
    far = n // 2 - reach
    pack_rows = up8(max(2 * slots, 4 * (slots - slots // 2)))
    chosen, affinity = [jnp.transpose(v, (2, 0, 1)) for v in (chosen, affinity)]
    lanes = max(128, 4 * n)
    dma, batches = pltpu.SemaphoreType.DMA, reach + far + 1
    vmem = pl.BlockSpec(memory_space=pltpu.VMEM)
    anywhere = pl.BlockSpec(memory_space=pl.ANY)
    return pl.pallas_call(
        functools.partial(kernel, n, reach, slots),
        out_shape=pltpu.VMEM((trows, half), bf16),
        in_specs=[anywhere] * 7,
        out_specs=vmem,
        scratch_shapes=[
            pltpu.VMEM((trows, model), bf16),
            pltpu.VMEM((1, model), f32),
            pltpu.VMEM(chosen.shape, jnp.int32),
            pltpu.VMEM(chosen.shape, f32),
            pltpu.VMEM((UNIT // 2, lanes), bf16),
            pltpu.VMEM((chunks, trows, width), bf16),
            pltpu.VMEM((2, reach, chunks, trows, width), bf16),
            pltpu.VMEM((2, reach, UNIT // 2, lanes), bf16),
            pltpu.VMEM((half, 2 * hid), bf16),
            pltpu.VMEM((half, 2 * hid), bf16),
            pltpu.VMEM((hid, half), bf16),
            pltpu.VMEM((hid, half), bf16),
            pltpu.VMEM((batches, 2 * UNIT, half), bf16),
            pltpu.VMEM((batches, 2 * UNIT, half), bf16),
            pltpu.VMEM((batches, 2 * UNIT, half), bf16),
            pltpu.VMEM((2, 2 * UNIT, half), bf16),
            pltpu.VMEM((2, 2 * UNIT, half), bf16),
            pltpu.VMEM((far, 2 * UNIT, half), bf16),
            pltpu.VMEM((far, 2 * UNIT, half), bf16),
            pltpu.VMEM((2, 2, far, pack_rows, width), bf16),
            pltpu.VMEM((2, 2, far, pack_rows, width), bf16),
            pltpu.VMEM((2, 2, far, pack_rows, width), bf16),
            pltpu.VMEM((2, 2, far, pack_rows, width), bf16),
            pltpu.VMEM((2, reach, chunks, trows, width), bf16),
            pltpu.VMEM((2, chunks, trows, width), bf16),
            dma((10,)),
            dma((2, reach, chunks)), dma((2, reach, chunks)),
            dma((2, reach)), dma((2, reach)),
            dma((batches,)), dma((batches,)), dma((batches,)), dma((batches,)),
            dma((2, 2, far)), dma((2, 2, far)), dma((2, 2, far)), dma((2, 2, far)),
            dma((2, reach, chunks)), dma((2, reach, chunks)),
        ],
        compiler_params=pltpu.CompilerParams(
            collective_id=0, has_side_effects=True, vmem_limit_bytes=58 * 2**20
        ),
    )(tokens, norm_gain[None, :], chosen, affinity, gate_weight, up_weight, down_weight)


def solution(mesh):
    n = mesh.shape["ep"]
    in_specs = (
        P(("grp", "ep"), None),
        P(),
        P("ep", None, "tp"),
        P("ep", None, "tp"),
        P("ep", "tp", None),
        P(("grp", "ep"), None, None),
        P(("grp", "ep"), None, None),
    )
    body = functools.partial(shards, n, min(REACH, n // 2 - 1), CHUNKS)
    return jax.shard_map(body, mesh=mesh, in_specs=in_specs, out_specs=P(("grp", "ep"), "tp"), check_vma=False)
```

```python
import functools

import jax
import jax.numpy as jnp
from jax import lax
from jax.experimental import pallas as pl
from jax.experimental.pallas import tpu as pltpu
from jax.sharding import PartitionSpec as P

norm_eps = 1e-06
UNIT = 32
REACH = 10
CHUNKS = 4
f32, bf16 = jnp.float32, jnp.bfloat16


def up8(rows):
    return -(-rows // 8) * 8


def dot(a, b):
    return jnp.dot(a, b, preferred_element_type=f32)


def dot_rows(a, b):
    return lax.dot_general(a, b, (((0,), (0,)), ((), ())), preferred_element_type=f32)


def kernel(
    n, reach, slots, tokens_hbm, gain_hbm, chosen_hbm, affinity_hbm, gate_hbm, up_hbm, down_hbm, out,
    tokens, gain, chosen, affinity, meta, own, ring, mring, w_own, w_oth, d_own, d_oth,
    pk_own, pk_oth, eo, ps, po, psf, pof, far_out, far_got, far_ret, far_in, red, top,
    wsem, dsend, drecv, msend, mrecv, pxs, pxr, pas, par, fs, fr, gs, gr, rs, rr,
):
    me, core = lax.axis_index("ep"), lax.axis_index("tp")
    far = n // 2 - reach
    chunks, trows, width = own.shape
    half = chunks * width
    hid = w_own.shape[1] // 2
    pack_rows = far_out.shape[3]
    batches = reach + far + 1
    partner = {"tp": 1 - core}
    sign = (1, -1)

    def at(offset):
        return {"ep": lax.rem(me + offset + n, n)}

    def rcopy(src, dst, s, r, dev):
        return pltpu.make_async_remote_copy(
            src_ref=src, dst_ref=dst, send_sem=s, recv_sem=r, device_id=dev,
            device_id_type=pl.DeviceIdType.MESH,
        )

    def hop(d, g, ch):
        src = own.at[ch] if d is None else ring.at[g, d, ch]
        nxt = 0 if d is None else d + 1
        return rcopy(src, ring.at[g, nxt, ch], dsend.at[g, nxt, ch], drecv.at[g, nxt, ch], at(sign[g]))

    def landed(d, g, ch):
        return rcopy(own.at[ch], ring.at[g, d, ch], dsend.at[g, d, ch], drecv.at[g, d, ch], at(sign[g]))

    def mhop(d, g):
        src = meta if d is None else mring.at[g, d]
        nxt = 0 if d is None else d + 1
        return rcopy(src, mring.at[g, nxt], msend.at[g, nxt], mrecv.at[g, nxt], at(sign[g]))

    def mlanded(d, g):
        return rcopy(meta, mring.at[g, d], msend.at[g, d], mrecv.at[g, d], at(sign[g]))

    def share(d):
        return rcopy(pk_own.at[d], pk_oth.at[d], pxs.at[d], pxr.at[d], partner)

    def give(src, d):
        return rcopy(src, eo.at[d], pas.at[d], par.at[d], partner)

    def far_copy(src, dst, s, r, g, j, h, way):
        return rcopy(
            src.at[g, h, j - 1], dst.at[g, h, j - 1], s.at[g, h, j - 1], r.at[g, h, j - 1], at(way * sign[g] * j)
        )

    def far_send(g, j, h):
        return far_copy(far_out, far_got, fs, fr, g, j, h, 1)

    def far_back(g, j, h):
        return far_copy(far_ret, far_in, gs, gr, g, j, h, -1)

    def parts_of(j):
        return (0,) if j == far else (0, 1)

    def back(src, d, g, ch):
        return rcopy(src, red.at[g, d, ch], rs.at[g, d, ch], rr.at[g, d, ch], at(-sign[g]))

    low = slots // 2
    lane = lax.broadcasted_iota(jnp.int32, meta.shape, 1)
    tok = lax.broadcasted_iota(jnp.int32, (UNIT, trows), 1).astype(f32)

    def column(m, index):
        pair = [jnp.sum(jnp.where(lane == index + 2 * n * i, m, 0.0), axis=1, keepdims=True) for i in range(2)]
        return jnp.concatenate(pair, axis=0)

    def hot(m, e, weighted):
        value = column(m, n + e) if weighted else 1.0
        return jnp.where(column(m, e) == tok, value, 0.0).astype(bf16)

    pack_r = lax.broadcasted_iota(jnp.int32, (pack_rows, UNIT), 0)
    pack_s = lax.broadcasted_iota(jnp.int32, (pack_rows, UNIT), 1)

    def packer(g, end, ch):
        count, first, place = slots, 0, ch % 2
        if end:
            count, first, place = (low, 0, ch) if g == 0 else (slots - low, low, ch)
        local = pack_r - place * count
        wanted = local + first
        wanted = jnp.where(wanted < low, wanted, wanted - low + UNIT // 2)
        keep = (local >= 0) & (local < count) & (pack_s == wanted)
        return jnp.where(keep, 1.0, 0.0).astype(bf16)

    def part(j, ch):
        return 0 if j == far else ch // 2

    def far_hot(m, g, weighted):
        hots = [hot(m, lax.rem(me + sign[g] * j + n, n), weighted) for j in range(1, far + 1)]
        sides = []
        for ch in range(2 if far > 1 else 0):
            pk = packer(g, False, ch)
            sides.append(jnp.concatenate([dot(pk, h) for h in hots[:-1]], axis=0).astype(bf16))
        ends = [dot(packer(g, True, ch), hots[-1]).astype(bf16) for ch in range(chunks)]
        return sides, ends

    barrier = pltpu.get_barrier_semaphore()
    peers = [at(1), at(-1), partner]
    for peer in peers:
        pl.semaphore_signal(barrier, inc=1, device_id=peer, device_id_type=pl.DeviceIdType.MESH)

    loads = []
    for i, (src, dst) in enumerate((
        (tokens_hbm, tokens),
        (gain_hbm, gain),
        (chosen_hbm, chosen),
        (affinity_hbm, affinity),
        (gate_hbm.at[0, pl.ds(core * half, half)], w_own.at[:, pl.ds(0, hid)]),
        (up_hbm.at[0, pl.ds(core * half, half)], w_own.at[:, pl.ds(hid, hid)]),
        (gate_hbm.at[0, pl.ds((1 - core) * half, half)], w_oth.at[:, pl.ds(0, hid)]),
        (up_hbm.at[0, pl.ds((1 - core) * half, half)], w_oth.at[:, pl.ds(hid, hid)]),
        (down_hbm.at[0, :, pl.ds(pl.multiple_of(core * half, 128), half)], d_own),
        (down_hbm.at[0, :, pl.ds(pl.multiple_of((1 - core) * half, 128), half)], d_oth),
    )):
        loads.append(pltpu.make_async_copy(src, dst, wsem.at[i]))
        loads[-1].start()

    loads[0].wait()
    loads[1].wait()
    squares = jnp.zeros((trows, 1), f32)
    for i in range(2 * chunks):
        v = tokens[:, pl.ds(i * width, width)].astype(f32)
        squares += jnp.sum(v * v, axis=1, keepdims=True)
    scale = lax.rsqrt(squares / tokens.shape[1] + norm_eps)
    for ch in range(chunks):
        cols = pl.ds(pl.multiple_of(core * half + ch * width, 128), width)
        own[ch] = (tokens[:, cols].astype(f32) * scale * gain[:, cols]).astype(bf16)
    loads[2].wait()
    loads[3].wait()
    experts = chosen.shape[2]
    s_row = lax.broadcasted_iota(jnp.int32, (meta.shape[0], slots), 0)
    s_col = lax.broadcasted_iota(jnp.int32, (meta.shape[0], slots), 1)
    e_row = lax.broadcasted_iota(jnp.int32, (experts, meta.shape[1]), 0)
    e_lane = lax.broadcasted_iota(jnp.int32, (experts, meta.shape[1]), 1)
    table = jnp.zeros(meta.shape, f32)
    for i, (first, count) in enumerate(((0, low), (low, slots - low))):
        spread = jnp.where((s_row < count) & (s_col == s_row + first), 1.0, 0.0).astype(bf16)
        dead = lax.broadcasted_iota(jnp.int32, meta.shape, 0) >= count
        table += jnp.where(dead & (lane >= 2 * n * i) & (lane < 2 * n * i + n), float(trows), 0.0)
        for ref, shift in ((chosen, 0), (affinity, n)):
            place = jnp.where(e_lane == e_row + shift + 2 * n * i, 1.0, 0.0).astype(bf16)
            moved = dot(ref[:, 0, :].astype(f32).astype(bf16), place).astype(bf16)
            table += dot(spread, moved)
    meta[...] = table.astype(bf16)
    pl.semaphore_wait(barrier, len(peers))

    for ch in range(chunks):
        for g in range(2):
            hop(None, g, ch).start()
            if ch == 0:
                mhop(None, g).start()
    pk_own[0, pl.ds(UNIT, UNIT)] = jnp.zeros_like(pk_own[0, pl.ds(UNIT, UNIT)])
    own_hot = hot(meta[...].astype(f32), me, False)
    for ch in range(chunks):
        pk_own[0, pl.ds(0, UNIT), pl.ds(ch * width, width)] = dot(own_hot, own[ch]).astype(bf16)
    share(0).start()
    for load in loads[4:]:
        load.wait()

    def hidden_of(a, b):
        acc = dot(a, w_own[...]) + dot(b, w_oth[...])
        gate, upper = acc[:, :hid], acc[:, hid:]
        return (gate * jax.nn.sigmoid(gate) * upper).astype(bf16)

    def pick(t):
        for g in range(2):
            h = hot(mring[g, t - 1].astype(f32), me, False)
            for ch in range(chunks):
                pk_own[t, pl.ds(g * UNIT, UNIT), pl.ds(ch * width, width)] = dot(h, ring[g, t - 1, ch]).astype(bf16)
        share(t).start()

    def pick_far(h):
        for g in range(2):
            sides, ends = far_hot(mring[g, reach - 1].astype(f32), g, False)
            if far > 1:
                y = dot(sides[0], ring[g, reach - 1, 2 * h]) + dot(sides[1], ring[g, reach - 1, 2 * h + 1])
                far_out[g, h, pl.ds(0, far - 1)] = y.astype(bf16).reshape(far - 1, pack_rows, width)
            if h == 1:
                y = sum(dot(ends[ch], ring[g, reach - 1, ch]) for ch in range(chunks))
                far_out[g, 0, far - 1] = y.astype(bf16)
        first = [(far - 1, 0)] if far > 1 else []
        rest = [(far, 0)] + ([(far - 1, 1)] if far > 1 else [])
        rest += [(j, p) for j in range(far - 2, 0, -1) for p in (0, 1)]
        for j, p in rest if h else first:
            for g in range(2):
                far_send(g, j, p).start()

    def expert(b):
        share(b).wait_recv()
        h = hidden_of(pk_own[b], pk_oth[b])
        spot = lax.rem(b, 2)

        @pl.when(b >= 2)
        def _():
            give(ps.at[spot], b - 2).wait_send()

        ps[spot] = dot(h, d_oth[...]).astype(bf16)
        give(ps.at[spot], b).start()
        po[spot] = dot(h, d_own[...]).astype(bf16)

    def finish(b):
        give(ps.at[0], b).wait_recv()
        eo[b] = (po[lax.rem(b, 2)].astype(f32) + eo[b].astype(f32)).astype(bf16)

    def step(t, carry):
        @pl.when(t <= reach)
        def _():
            for g in range(2):
                mlanded(t - 1, g).wait_recv()

                @pl.when(t < reach)
                def _():
                    mhop(t - 1, g).start()

        for ch in range(chunks):
            @pl.when(t <= reach)
            def _():
                for g in range(2):
                    landed(t - 1, g, ch).wait_recv()

                    @pl.when(t < reach)
                    def _():
                        hop(t - 1, g, ch).start()

            if ch % 2:
                @pl.when(t == reach)
                def _():
                    pick_far(ch // 2)

            if ch == 0:
                @pl.when(t <= reach + 1)
                def _():
                    expert(t - 1)

            if ch == chunks - 2:
                @pl.when(t >= 2)
                def _():
                    finish(t - 2)

        @pl.when(t <= reach)
        def _():
            pick(t)

        return carry

    lax.fori_loop(1, reach + 3, step, 0)

    def far_arrive(js):
        for j in js:
            for g in range(2):
                for p in parts_of(j):
                    far_send(g, j, p).wait_recv()
            for g in range(2):
                for ch in range(chunks):
                    rows = dot_rows(packer(g, j == far, ch), far_got[g, part(j, ch), j - 1])
                    pk_own[reach + j, pl.ds(g * UNIT, UNIT), pl.ds(ch * width, width)] = rows.astype(bf16)
            share(reach + j).start()

    def far_experts(js):
        for j in js:
            share(reach + j).wait_recv()
        least, count = min(js), len(js)
        group, rows = pl.ds(reach + least, count), count * 2 * UNIT
        h = hidden_of(pk_own[group].reshape(rows, half), pk_oth[group].reshape(rows, half))
        spots = pl.ds(least - 1, count)
        psf[spots] = dot(h, d_oth[...]).astype(bf16).reshape(count, 2 * UNIT, half)
        for j in js:
            give(psf.at[j - 1], reach + j).start()
        pof[spots] = dot(h, d_own[...]).astype(bf16).reshape(count, 2 * UNIT, half)
        for j in js:
            b = reach + j
            give(psf.at[j - 1], b).wait_recv()
            eo[b] = (pof[j - 1].astype(f32) + eo[b].astype(f32)).astype(bf16)
            for g in range(2):
                for p in parts_of(j):
                    y = jnp.zeros((pack_rows, width), f32)
                    for ch in range(chunks):
                        if part(j, ch) == p:
                            y += dot(packer(g, j == far, ch), eo[b, pl.ds(g * UNIT, UNIT), pl.ds(ch * width, width)])
                    far_ret[g, p, j - 1] = y.astype(bf16)

    def far_return(js, p):
        for j in js:
            if p in parts_of(j):
                for g in range(2):
                    far_back(g, j, p).start()

    order = list(range(far, 0, -1))
    groups = [order[:2], order[2:-2], order[-2:]] if far > 4 else [order]
    held = []
    for i, js in enumerate(groups):
        far_arrive(js)
        far_return(held[:1], 1)
        far_experts(js)
        far_return(js, 0)
        far_return(held[1:], 1)
        held = js
        if i < len(groups) - 2:
            far_return(js, 1)
            held = []
    far_return(held, 1)

    own_w = hot(meta[...].astype(f32), me, True)
    near_w = [hot(mring[g, reach - 1].astype(f32), me, True) for g in range(2)]
    far_w = [far_hot(mring[g, reach - 1].astype(f32), g, True) for g in range(2)]
    for h in range(2):
        for j in order:
            if h in parts_of(j):
                for g in range(2):
                    far_back(g, j, h).wait_recv()
        for ch in (2 * h, 2 * h + 1):
            cols = pl.ds(ch * width, width)
            for g in range(2):
                sides, ends = far_w[g]
                total = dot_rows(near_w[g], eo[reach, pl.ds(g * UNIT, UNIT), cols])
                total += dot_rows(ends[ch], far_in[g, 0, far - 1])
                if far > 1:
                    total += dot_rows(sides[ch % 2], far_in[g, h, pl.ds(0, far - 1)].reshape((far - 1) * pack_rows, width))
                top[g, ch] = total.astype(bf16)
                back(top.at[g, ch], reach - 1, g, ch).start()

    def fold(i, carry):
        d = reach - i
        hots = [hot(mring[g, d - 1].astype(f32), me, True) for g in range(2)]
        for ch in range(chunks):
            cols = pl.ds(ch * width, width)
            for g in range(2):
                add = dot_rows(hots[g], eo[d, pl.ds(g * UNIT, UNIT), cols])
                back(top.at[g, ch], d, g, ch).wait_recv()
                red[g, d, ch] = (red[g, d, ch].astype(f32) + add).astype(bf16)
                back(red.at[g, d, ch], d - 1, g, ch).start()
        return carry

    lax.fori_loop(1, reach, fold, 0)

    for ch in range(chunks):
        cols = pl.ds(ch * width, width)
        add = dot_rows(own_w, eo[0, pl.ds(0, UNIT), cols])
        for g in range(2):
            back(top.at[g, ch], 0, g, ch).wait_recv()
            add += red[g, 0, ch].astype(f32)
        out[:, cols] = add.astype(bf16)

    def drain(d, carry):
        for g in range(2):
            mlanded(d, g).wait_send()
            for ch in range(chunks):
                landed(d, g, ch).wait_send()
                back(top.at[g, ch], d, g, ch).wait_send()
        return carry

    lax.fori_loop(0, reach, drain, 0)

    def drain_share(d, carry):
        share(d).wait_send()
        return carry

    lax.fori_loop(0, batches, drain_share, 0)
    for b in (reach - 1, reach):
        give(ps.at[0], b).wait_send()
    for j in order:
        give(psf.at[j - 1], reach + j).wait_send()
        for g in range(2):
            for p in parts_of(j):
                far_send(g, j, p).wait_send()
                far_back(g, j, p).wait_send()


def shards(n, reach, chunks, tokens, norm_gain, gate_weight, up_weight, down_weight, chosen, affinity):
    trows, model = tokens.shape
    half = model // 2
    width = half // chunks
    slots = chosen.shape[2]
    hid = gate_weight.shape[2]
    far = n // 2 - reach
    pack_rows = up8(max(2 * slots, 4 * (slots - slots // 2)))
    chosen, affinity = [jnp.transpose(v, (2, 0, 1)) for v in (chosen, affinity)]
    lanes = max(128, 4 * n)
    dma, batches = pltpu.SemaphoreType.DMA, reach + far + 1
    vmem = pl.BlockSpec(memory_space=pltpu.VMEM)
    anywhere = pl.BlockSpec(memory_space=pl.ANY)
    return pl.pallas_call(
        functools.partial(kernel, n, reach, slots),
        out_shape=pltpu.VMEM((trows, half), bf16),
        in_specs=[anywhere] * 7,
        out_specs=vmem,
        scratch_shapes=[
            pltpu.VMEM((trows, model), bf16),
            pltpu.VMEM((1, model), f32),
            pltpu.VMEM(chosen.shape, jnp.int32),
            pltpu.VMEM(chosen.shape, f32),
            pltpu.VMEM((UNIT // 2, lanes), bf16),
            pltpu.VMEM((chunks, trows, width), bf16),
            pltpu.VMEM((2, reach, chunks, trows, width), bf16),
            pltpu.VMEM((2, reach, UNIT // 2, lanes), bf16),
            pltpu.VMEM((half, 2 * hid), bf16),
            pltpu.VMEM((half, 2 * hid), bf16),
            pltpu.VMEM((hid, half), bf16),
            pltpu.VMEM((hid, half), bf16),
            pltpu.VMEM((batches, 2 * UNIT, half), bf16),
            pltpu.VMEM((batches, 2 * UNIT, half), bf16),
            pltpu.VMEM((batches, 2 * UNIT, half), bf16),
            pltpu.VMEM((2, 2 * UNIT, half), bf16),
            pltpu.VMEM((2, 2 * UNIT, half), bf16),
            pltpu.VMEM((far, 2 * UNIT, half), bf16),
            pltpu.VMEM((far, 2 * UNIT, half), bf16),
            pltpu.VMEM((2, 2, far, pack_rows, width), bf16),
            pltpu.VMEM((2, 2, far, pack_rows, width), bf16),
            pltpu.VMEM((2, 2, far, pack_rows, width), bf16),
            pltpu.VMEM((2, 2, far, pack_rows, width), bf16),
            pltpu.VMEM((2, reach, chunks, trows, width), bf16),
            pltpu.VMEM((2, chunks, trows, width), bf16),
            dma((10,)),
            dma((2, reach, chunks)), dma((2, reach, chunks)),
            dma((2, reach)), dma((2, reach)),
            dma((batches,)), dma((batches,)), dma((batches,)), dma((batches,)),
            dma((2, 2, far)), dma((2, 2, far)), dma((2, 2, far)), dma((2, 2, far)),
            dma((2, reach, chunks)), dma((2, reach, chunks)),
        ],
        compiler_params=pltpu.CompilerParams(
            collective_id=0, has_side_effects=True, vmem_limit_bytes=58 * 2**20
        ),
    )(tokens, norm_gain[None, :], chosen, affinity, gate_weight, up_weight, down_weight)


def solution(mesh):
    n = mesh.shape["ep"]
    in_specs = (
        P(("grp", "ep"), None),
        P(),
        P("ep", None, "tp"),
        P("ep", None, "tp"),
        P("ep", "tp", None),
        P(("grp", "ep"), None, None),
        P(("grp", "ep"), None, None),
    )
    body = functools.partial(shards, n, min(REACH, n // 2 - 1), CHUNKS)
    return jax.shard_map(body, mesh=mesh, in_specs=in_specs, out_specs=P(("grp", "ep"), "tp"), check_vma=False)
```

```python
import functools

import jax
import jax.numpy as jnp
from jax import lax
from jax.experimental import pallas as pl
from jax.experimental.pallas import tpu as pltpu
from jax.sharding import PartitionSpec as P

norm_eps = 1e-06
UNIT = 32
REACH = 10
CHUNKS = 4
f32, bf16 = jnp.float32, jnp.bfloat16


def up8(rows):
    return -(-rows // 8) * 8


def dot(a, b):
    return jnp.dot(a, b, preferred_element_type=f32)


def dot_rows(a, b):
    return lax.dot_general(a, b, (((0,), (0,)), ((), ())), preferred_element_type=f32)


def kernel(
    n, reach, slots, tokens_hbm, gain_hbm, chosen_hbm, affinity_hbm, gate_hbm, up_hbm, down_hbm, out,
    tokens, gain, chosen, affinity, meta, own, ring, mring, w_own, w_oth, d_own, d_oth,
    pk_own, pk_oth, eo, ps, po, psf, pof, far_out, far_got, far_ret, far_in, red, top,
    wsem, dsend, drecv, msend, mrecv, pxs, pxr, pas, par, fs, fr, gs, gr, rs, rr,
):
    me, core = lax.axis_index("ep"), lax.axis_index("tp")
    far = n // 2 - reach
    chunks, trows, width = own.shape
    half = chunks * width
    hid = w_own.shape[1] // 2
    pack_rows = far_out.shape[3]
    batches = reach + far + 1
    partner = {"tp": 1 - core}
    sign = (1, -1)

    def at(offset):
        return {"ep": lax.rem(me + offset + n, n)}

    def rcopy(src, dst, s, r, dev):
        return pltpu.make_async_remote_copy(
            src_ref=src, dst_ref=dst, send_sem=s, recv_sem=r, device_id=dev,
            device_id_type=pl.DeviceIdType.MESH,
        )

    def hop(d, g, ch):
        src = own.at[ch] if d is None else ring.at[g, d, ch]
        nxt = 0 if d is None else d + 1
        return rcopy(src, ring.at[g, nxt, ch], dsend.at[g, nxt, ch], drecv.at[g, nxt, ch], at(sign[g]))

    def landed(d, g, ch):
        return rcopy(own.at[ch], ring.at[g, d, ch], dsend.at[g, d, ch], drecv.at[g, d, ch], at(sign[g]))

    def mhop(d, g):
        src = meta if d is None else mring.at[g, d]
        nxt = 0 if d is None else d + 1
        return rcopy(src, mring.at[g, nxt], msend.at[g, nxt], mrecv.at[g, nxt], at(sign[g]))

    def mlanded(d, g):
        return rcopy(meta, mring.at[g, d], msend.at[g, d], mrecv.at[g, d], at(sign[g]))

    def share(d):
        return rcopy(pk_own.at[d], pk_oth.at[d], pxs.at[d], pxr.at[d], partner)

    def give(src, d):
        return rcopy(src, eo.at[d], pas.at[d], par.at[d], partner)

    def far_copy(src, dst, s, r, g, j, h, way):
        return rcopy(
            src.at[g, h, j - 1], dst.at[g, h, j - 1], s.at[g, h, j - 1], r.at[g, h, j - 1], at(way * sign[g] * j)
        )

    def far_send(g, j, h):
        return far_copy(far_out, far_got, fs, fr, g, j, h, 1)

    def far_back(g, j, h):
        return far_copy(far_ret, far_in, gs, gr, g, j, h, -1)

    def parts_of(j):
        return (0,) if j == far else (0, 1)

    def back(src, d, g, ch):
        return rcopy(src, red.at[g, d, ch], rs.at[g, d, ch], rr.at[g, d, ch], at(-sign[g]))

    low = slots // 2
    lane = lax.broadcasted_iota(jnp.int32, meta.shape, 1)
    tok = lax.broadcasted_iota(jnp.int32, (UNIT, trows), 1).astype(f32)

    def column(m, index):
        pair = [jnp.sum(jnp.where(lane == index + 2 * n * i, m, 0.0), axis=1, keepdims=True) for i in range(2)]
        return jnp.concatenate(pair, axis=0)

    def hot(m, e, weighted):
        value = column(m, n + e) if weighted else 1.0
        return jnp.where(column(m, e) == tok, value, 0.0).astype(bf16)

    pack_r = lax.broadcasted_iota(jnp.int32, (pack_rows, UNIT), 0)
    pack_s = lax.broadcasted_iota(jnp.int32, (pack_rows, UNIT), 1)

    def packer(g, end, ch):
        count, first, place = slots, 0, ch % 2
        if end:
            count, first, place = (low, 0, ch) if g == 0 else (slots - low, low, ch)
        local = pack_r - place * count
        wanted = local + first
        wanted = jnp.where(wanted < low, wanted, wanted - low + UNIT // 2)
        keep = (local >= 0) & (local < count) & (pack_s == wanted)
        return jnp.where(keep, 1.0, 0.0).astype(bf16)

    def part(j, ch):
        return 0 if j == far else ch // 2

    def far_hot(m, g, weighted):
        hots = [hot(m, lax.rem(me + sign[g] * j + n, n), weighted) for j in range(1, far + 1)]
        sides = []
        for ch in range(2 if far > 1 else 0):
            pk = packer(g, False, ch)
            sides.append(jnp.concatenate([dot(pk, h) for h in hots[:-1]], axis=0).astype(bf16))
        ends = [dot(packer(g, True, ch), hots[-1]).astype(bf16) for ch in range(chunks)]
        return sides, ends

    barrier = pltpu.get_barrier_semaphore()
    peers = [at(1), at(-1), partner]
    for peer in peers:
        pl.semaphore_signal(barrier, inc=1, device_id=peer, device_id_type=pl.DeviceIdType.MESH)

    loads = []
    for i, (src, dst) in enumerate((
        (tokens_hbm, tokens),
        (gain_hbm, gain),
        (chosen_hbm, chosen),
        (affinity_hbm, affinity),
        (gate_hbm.at[0, pl.ds(core * half, half)], w_own.at[:, pl.ds(0, hid)]),
        (up_hbm.at[0, pl.ds(core * half, half)], w_own.at[:, pl.ds(hid, hid)]),
        (gate_hbm.at[0, pl.ds((1 - core) * half, half)], w_oth.at[:, pl.ds(0, hid)]),
        (up_hbm.at[0, pl.ds((1 - core) * half, half)], w_oth.at[:, pl.ds(hid, hid)]),
        (down_hbm.at[0, :, pl.ds(pl.multiple_of(core * half, 128), half)], d_own),
        (down_hbm.at[0, :, pl.ds(pl.multiple_of((1 - core) * half, 128), half)], d_oth),
    )):
        loads.append(pltpu.make_async_copy(src, dst, wsem.at[i]))
        loads[-1].start()

    loads[0].wait()
    loads[1].wait()
    squares = jnp.zeros((trows, 1), f32)
    for i in range(2 * chunks):
        v = tokens[:, pl.ds(i * width, width)].astype(f32)
        squares += jnp.sum(v * v, axis=1, keepdims=True)
    scale = lax.rsqrt(squares / tokens.shape[1] + norm_eps)
    for ch in range(chunks):
        cols = pl.ds(pl.multiple_of(core * half + ch * width, 128), width)
        own[ch] = (tokens[:, cols].astype(f32) * scale * gain[:, cols]).astype(bf16)
    loads[2].wait()
    loads[3].wait()
    experts = chosen.shape[2]
    s_row = lax.broadcasted_iota(jnp.int32, (meta.shape[0], slots), 0)
    s_col = lax.broadcasted_iota(jnp.int32, (meta.shape[0], slots), 1)
    e_row = lax.broadcasted_iota(jnp.int32, (experts, meta.shape[1]), 0)
    e_lane = lax.broadcasted_iota(jnp.int32, (experts, meta.shape[1]), 1)
    table = jnp.zeros(meta.shape, f32)
    for i, (first, count) in enumerate(((0, low), (low, slots - low))):
        spread = jnp.where((s_row < count) & (s_col == s_row + first), 1.0, 0.0).astype(bf16)
        dead = lax.broadcasted_iota(jnp.int32, meta.shape, 0) >= count
        table += jnp.where(dead & (lane >= 2 * n * i) & (lane < 2 * n * i + n), float(trows), 0.0)
        for ref, shift in ((chosen, 0), (affinity, n)):
            place = jnp.where(e_lane == e_row + shift + 2 * n * i, 1.0, 0.0).astype(bf16)
            moved = dot(ref[:, 0, :].astype(f32).astype(bf16), place).astype(bf16)
            table += dot(spread, moved)
    meta[...] = table.astype(bf16)
    pl.semaphore_wait(barrier, len(peers))

    for ch in range(chunks):
        for g in range(2):
            hop(None, g, ch).start()
            if ch == 0:
                mhop(None, g).start()
    pk_own[0, pl.ds(UNIT, UNIT)] = jnp.zeros_like(pk_own[0, pl.ds(UNIT, UNIT)])
    own_hot = hot(meta[...].astype(f32), me, False)
    for ch in range(chunks):
        pk_own[0, pl.ds(0, UNIT), pl.ds(ch * width, width)] = dot(own_hot, own[ch]).astype(bf16)
    share(0).start()
    for load in loads[4:]:
        load.wait()

    def hidden_of(a, b):
        acc = dot(a, w_own[...]) + dot(b, w_oth[...])
        gate, upper = acc[:, :hid], acc[:, hid:]
        return (gate * jax.nn.sigmoid(gate) * upper).astype(bf16)

    def pick(t):
        for g in range(2):
            h = hot(mring[g, t - 1].astype(f32), me, False)
            for ch in range(chunks):
                pk_own[t, pl.ds(g * UNIT, UNIT), pl.ds(ch * width, width)] = dot(h, ring[g, t - 1, ch]).astype(bf16)
        share(t).start()

    def pick_far(h):
        for g in range(2):
            sides, ends = far_hot(mring[g, reach - 1].astype(f32), g, False)
            if far > 1:
                y = dot(sides[0], ring[g, reach - 1, 2 * h]) + dot(sides[1], ring[g, reach - 1, 2 * h + 1])
                far_out[g, h, pl.ds(0, far - 1)] = y.astype(bf16).reshape(far - 1, pack_rows, width)
            if h == 1:
                y = sum(dot(ends[ch], ring[g, reach - 1, ch]) for ch in range(chunks))
                far_out[g, 0, far - 1] = y.astype(bf16)
        first = [(far - 1, 0)] if far > 1 else []
        rest = [(far, 0)] + ([(far - 1, 1)] if far > 1 else [])
        rest += [(j, p) for j in range(far - 2, 0, -1) for p in (0, 1)]
        for j, p in rest if h else first:
            for g in range(2):
                far_send(g, j, p).start()

    def expert(b):
        share(b).wait_recv()
        h = hidden_of(pk_own[b], pk_oth[b])
        spot = lax.rem(b, 2)

        @pl.when(b >= 2)
        def _():
            give(ps.at[spot], b - 2).wait_send()

        ps[spot] = dot(h, d_oth[...]).astype(bf16)
        give(ps.at[spot], b).start()
        po[spot] = dot(h, d_own[...]).astype(bf16)

    def finish(b):
        give(ps.at[0], b).wait_recv()
        eo[b] = (po[lax.rem(b, 2)].astype(f32) + eo[b].astype(f32)).astype(bf16)

    def step(t, carry):
        @pl.when(t <= reach)
        def _():
            for g in range(2):
                mlanded(t - 1, g).wait_recv()

                @pl.when(t < reach)
                def _():
                    mhop(t - 1, g).start()

        for ch in range(chunks):
            @pl.when(t <= reach)
            def _():
                for g in range(2):
                    landed(t - 1, g, ch).wait_recv()

                    @pl.when(t < reach)
                    def _():
                        hop(t - 1, g, ch).start()

            if ch % 2:
                @pl.when(t == reach)
                def _():
                    pick_far(ch // 2)

            if ch == 0:
                @pl.when(t <= reach + 1)
                def _():
                    expert(t - 1)

            if ch == chunks - 2:
                @pl.when(t >= 2)
                def _():
                    finish(t - 2)

        @pl.when(t <= reach)
        def _():
            pick(t)

        return carry

    lax.fori_loop(1, reach + 3, step, 0)

    def far_arrive(js):
        for j in js:
            for g in range(2):
                for p in parts_of(j):
                    far_send(g, j, p).wait_recv()
            for g in range(2):
                for ch in range(chunks):
                    rows = dot_rows(packer(g, j == far, ch), far_got[g, part(j, ch), j - 1])
                    pk_own[reach + j, pl.ds(g * UNIT, UNIT), pl.ds(ch * width, width)] = rows.astype(bf16)
            share(reach + j).start()

    def far_experts(js):
        for j in js:
            share(reach + j).wait_recv()
        least, count = min(js), len(js)
        group, rows = pl.ds(reach + least, count), count * 2 * UNIT
        h = hidden_of(pk_own[group].reshape(rows, half), pk_oth[group].reshape(rows, half))
        spots = pl.ds(least - 1, count)
        psf[spots] = dot(h, d_oth[...]).astype(bf16).reshape(count, 2 * UNIT, half)
        for j in js:
            give(psf.at[j - 1], reach + j).start()
        pof[spots] = dot(h, d_own[...]).astype(bf16).reshape(count, 2 * UNIT, half)
        for j in js:
            b = reach + j
            give(psf.at[j - 1], b).wait_recv()
            eo[b] = (pof[j - 1].astype(f32) + eo[b].astype(f32)).astype(bf16)
            for g in range(2):
                for p in parts_of(j):
                    y = jnp.zeros((pack_rows, width), f32)
                    for ch in range(chunks):
                        if part(j, ch) == p:
                            y += dot(packer(g, j == far, ch), eo[b, pl.ds(g * UNIT, UNIT), pl.ds(ch * width, width)])
                    far_ret[g, p, j - 1] = y.astype(bf16)

    def far_return(js, p):
        for j in js:
            if p in parts_of(j):
                for g in range(2):
                    far_back(g, j, p).start()

    order = list(range(far, 0, -1))
    groups = [order[:2], order[2:-2], order[-2:]] if far > 4 else [order]
    last = groups[-1]

    def far_left():
        for j in last:
            for g in range(2):
                for p in parts_of(j):
                    far_send(g, j, p).wait_send()

    if len(groups) == 1:
        far_arrive(last)
        far_left()
        far_experts(last)
    else:
        far_arrive(groups[0])
        far_experts(groups[0])
        far_arrive(groups[1])
        far_left()
        far_return(groups[0], 0)
        far_return(groups[0], 1)
        far_experts(groups[1])
        far_return(groups[1], 0)
        far_return(groups[1][:1], 1)
        far_arrive(last)
        far_experts(last)
    far_return(last, 0)
    if len(groups) > 1:
        far_return(groups[1][1:], 1)
    far_return(last, 1)

    own_w = hot(meta[...].astype(f32), me, True)
    near_w = [hot(mring[g, reach - 1].astype(f32), me, True) for g in range(2)]
    far_w = [far_hot(mring[g, reach - 1].astype(f32), g, True) for g in range(2)]
    for h in range(2):
        for j in order:
            if h in parts_of(j):
                for g in range(2):
                    far_back(g, j, h).wait_recv()
        for ch in (2 * h, 2 * h + 1):
            cols = pl.ds(ch * width, width)
            for g in range(2):
                sides, ends = far_w[g]
                total = dot_rows(near_w[g], eo[reach, pl.ds(g * UNIT, UNIT), cols])
                total += dot_rows(ends[ch], far_in[g, 0, far - 1])
                if far > 1:
                    total += dot_rows(sides[ch % 2], far_in[g, h, pl.ds(0, far - 1)].reshape((far - 1) * pack_rows, width))
                top[g, ch] = total.astype(bf16)
                back(top.at[g, ch], reach - 1, g, ch).start()

    def fold(i, carry):
        d = reach - i
        hots = [hot(mring[g, d - 1].astype(f32), me, True) for g in range(2)]
        for ch in range(chunks):
            cols = pl.ds(ch * width, width)
            for g in range(2):
                add = dot_rows(hots[g], eo[d, pl.ds(g * UNIT, UNIT), cols])
                back(top.at[g, ch], d, g, ch).wait_recv()
                red[g, d, ch] = (red[g, d, ch].astype(f32) + add).astype(bf16)
                back(red.at[g, d, ch], d - 1, g, ch).start()
        return carry

    lax.fori_loop(1, reach, fold, 0)

    for ch in range(chunks):
        cols = pl.ds(ch * width, width)
        add = dot_rows(own_w, eo[0, pl.ds(0, UNIT), cols])
        for g in range(2):
            back(top.at[g, ch], 0, g, ch).wait_recv()
            add += red[g, 0, ch].astype(f32)
        out[:, cols] = add.astype(bf16)

    def drain(d, carry):
        for g in range(2):
            mlanded(d, g).wait_send()
            for ch in range(chunks):
                landed(d, g, ch).wait_send()
                back(top.at[g, ch], d, g, ch).wait_send()
        return carry

    lax.fori_loop(0, reach, drain, 0)

    def drain_share(d, carry):
        share(d).wait_send()
        return carry

    lax.fori_loop(0, batches, drain_share, 0)
    for b in (reach - 1, reach):
        give(ps.at[0], b).wait_send()
    for j in order:
        give(psf.at[j - 1], reach + j).wait_send()
        for g in range(2):
            for p in parts_of(j):
                if j not in last:
                    far_send(g, j, p).wait_send()
                far_back(g, j, p).wait_send()


def shards(n, reach, chunks, tokens, norm_gain, gate_weight, up_weight, down_weight, chosen, affinity):
    trows, model = tokens.shape
    half = model // 2
    width = half // chunks
    slots = chosen.shape[2]
    hid = gate_weight.shape[2]
    far = n // 2 - reach
    pack_rows = up8(max(2 * slots, 4 * (slots - slots // 2)))
    chosen, affinity = [jnp.transpose(v, (2, 0, 1)) for v in (chosen, affinity)]
    lanes = max(128, 4 * n)
    dma, batches = pltpu.SemaphoreType.DMA, reach + far + 1
    vmem = pl.BlockSpec(memory_space=pltpu.VMEM)
    anywhere = pl.BlockSpec(memory_space=pl.ANY)
    return pl.pallas_call(
        functools.partial(kernel, n, reach, slots),
        out_shape=pltpu.VMEM((trows, half), bf16),
        in_specs=[anywhere] * 7,
        out_specs=vmem,
        scratch_shapes=[
            pltpu.VMEM((trows, model), bf16),
            pltpu.VMEM((1, model), f32),
            pltpu.VMEM(chosen.shape, jnp.int32),
            pltpu.VMEM(chosen.shape, f32),
            pltpu.VMEM((UNIT // 2, lanes), bf16),
            pltpu.VMEM((chunks, trows, width), bf16),
            pltpu.VMEM((2, reach, chunks, trows, width), bf16),
            pltpu.VMEM((2, reach, UNIT // 2, lanes), bf16),
            pltpu.VMEM((half, 2 * hid), bf16),
            pltpu.VMEM((half, 2 * hid), bf16),
            pltpu.VMEM((hid, half), bf16),
            pltpu.VMEM((hid, half), bf16),
            pltpu.VMEM((batches, 2 * UNIT, half), bf16),
            pltpu.VMEM((batches, 2 * UNIT, half), bf16),
            pltpu.VMEM((batches, 2 * UNIT, half), bf16),
            pltpu.VMEM((2, 2 * UNIT, half), bf16),
            pltpu.VMEM((2, 2 * UNIT, half), bf16),
            pltpu.VMEM((far, 2 * UNIT, half), bf16),
            pltpu.VMEM((far, 2 * UNIT, half), bf16),
            pltpu.VMEM((2, 2, far, pack_rows, width), bf16),
            pltpu.VMEM((2, 2, far, pack_rows, width), bf16),
            pltpu.VMEM((2, 2, far, pack_rows, width), bf16),
            pltpu.VMEM((2, 2, far, pack_rows, width), bf16),
            pltpu.VMEM((2, reach, chunks, trows, width), bf16),
            pltpu.VMEM((2, chunks, trows, width), bf16),
            dma((10,)),
            dma((2, reach, chunks)), dma((2, reach, chunks)),
            dma((2, reach)), dma((2, reach)),
            dma((batches,)), dma((batches,)), dma((batches,)), dma((batches,)),
            dma((2, 2, far)), dma((2, 2, far)), dma((2, 2, far)), dma((2, 2, far)),
            dma((2, reach, chunks)), dma((2, reach, chunks)),
        ],
        compiler_params=pltpu.CompilerParams(
            collective_id=0, has_side_effects=True, vmem_limit_bytes=58 * 2**20
        ),
    )(tokens, norm_gain[None, :], chosen, affinity, gate_weight, up_weight, down_weight)


def solution(mesh):
    n = mesh.shape["ep"]
    in_specs = (
        P(("grp", "ep"), None),
        P(),
        P("ep", None, "tp"),
        P("ep", None, "tp"),
        P("ep", "tp", None),
        P(("grp", "ep"), None, None),
        P(("grp", "ep"), None, None),
    )
    body = functools.partial(shards, n, min(REACH, n // 2 - 1), CHUNKS)
    return jax.shard_map(body, mesh=mesh, in_specs=in_specs, out_specs=P(("grp", "ep"), "tp"), check_vma=False)
```
